256 devices in a mesh: sp: 64 (over z, y, core), tp: 4 (over x).
Axes of the slice: x: 4, y: 4, z: 8, core: 2. Of those that a mesh axis runs over, the one named last changes fastest.
Arguments:
- tokens: bfloat16 [10240, 2048], P('sp'), may hold values from -6 to 6
- input_gain: float32 [2048], replicated, may hold values from 0.1 to 1.9
- chain_query: bfloat16 [2048, 1024], P('sp', 'tp'), may hold values from -0.125 to 0.125
- forward_gate: bfloat16 [2048, 1024], P('sp', 'tp'), may hold values from -0.125 to 0.125
- backward_gate: bfloat16 [2048, 1024], P('sp', 'tp'), may hold values from -0.125 to 0.125
- chain_value: bfloat16 [2048, 1024], P('sp', 'tp'), may hold values from -0.125 to 0.125
- output_gate: bfloat16 [2048, 1024], P('sp', 'tp'), may hold values from -0.125 to 0.125
- forget_rate: float32 [2, 1024], P(None, 'tp'), may hold values from 0.2 to 6
- chain_gain: float32 [1024], P('tp'), may hold values from 0.1 to 1.9
- query_down: bfloat16 [2048, 768], P('sp'), may hold values from -0.125 to 0.125
- latent_down: bfloat16 [2048, 512], P('sp'), may hold values from -0.125 to 0.125
- rotary_down: bfloat16 [2048, 64], replicated, may hold values from -0.125 to 0.125
- query_latent_gain: float32 [768], replicated, may hold values from 0.1 to 1.9
- latent_gain: float32 [512], replicated, may hold values from 0.1 to 1.9
- query_up: bfloat16 [768, 1536], P(None, 'tp'), may hold values from -0.21875 to 0.21875
- latent_up: bfloat16 [512, 2048], P(None, 'tp'), may hold values from -0.25 to 0.25
- query_head_gain: float32 [192], replicated, may hold values from 0.1 to 1.9
- key_head_gain: float32 [192], replicated, may hold values from 0.1 to 1.9
- mixer_gain: float32 [1024], P('tp'), may hold values from 0.1 to 1.9
- chain_out: bfloat16 [1024, 2048], P('tp', 'sp'), may hold values from -0.125 to 0.125
- attend_out: bfloat16 [1024, 2048], P('tp', 'sp'), may hold values from -0.125 to 0.125
Outputs:
- mixed: float32 [10240, 2048], P(('sp', 'tp'))
The draws below stay inside these ranges and needn't reach their ends.
All inputs are finite; a program needn't handle non-finite values.
Results may differ from the reference program's by a relative error of at most 0.017.
Values may be sent and summed in bfloat16 or wider, within the bound.
No kernel may reach another device: no remote copies, remote signals or barrier semaphores. Data moves between devices by JAX's collectives and lax.ppermute only.
A program may use at most 128 MiB of HBM per device.

```python
import math
import jax
import jax.numpy as jnp
from jax import lax

D = 2048
KEY_DIM = 128
VAL_DIM = 128
HEADS_ATT = 8
NOPE_DIM = 128
ROPE_DIM = 64
VHEAD_DIM = 128
QLAT = 768
KVLAT = 512
TOK_DEV = 160
SEQ = 10240
REC_KEYS = 1024
REC_WIDTH = 1024
ATT_QK = 192
ATT_WIDTH = 1024


def block_levels(key, shape, cuts, low, top_value):
    factor_of = 1.0
    for dim, parts in cuts:
        draws = jax.random.uniform(jax.random.fold_in(jax.random.fold_in(key, 6), dim), (parts,), jnp.float32, low / len(cuts), top_value / len(cuts))
        factor_of = factor_of * jnp.repeat(jnp.exp(draws), shape[dim] // parts).reshape((-1,) + (1,) * (len(shape) - 1 - dim))
    return factor_of


def normal_values(stream_key, extent, width, bound, cuts=(), held_as=jnp.bfloat16):
    loudness = block_levels(stream_key, extent, cuts, -0.22, 0.18) if cuts else 1.0
    entries = jax.random.normal(stream_key, extent, jnp.float32) * width * loudness
    return jnp.minimum(jnp.maximum(entries, -bound), bound).astype(held_as)


def setup_inputs(seed: int = 0) -> dict:
    key_list = jax.random.split(jax.random.key(seed), 22)
    tokens = normal_values(key_list[0], (SEQ, D), 1.0, 6.0, ((0, 64),))
    input_gain = jnp.clip(1.0 + 0.18 * jax.random.normal(key_list[1], (D,), jnp.float32), 0.1, 1.9)
    chain_query = normal_values(key_list[2], (D, REC_KEYS), D ** -0.5, 0.125, ((0, 64), (1, 4)))
    forward_gate = normal_values(key_list[3], (D, REC_KEYS), D ** -0.5, 0.125, ((0, 64), (1, 4)))
    backward_gate = normal_values(key_list[4], (D, REC_KEYS), D ** -0.5, 0.125, ((0, 64), (1, 4)))
    chain_value = normal_values(key_list[5], (D, REC_WIDTH), D ** -0.5, 0.125, ((0, 64), (1, 4)))
    output_gate = normal_values(key_list[6], (D, REC_WIDTH), D ** -0.5, 0.125, ((0, 64), (1, 4)))
    forget_rate = jnp.clip(jnp.exp(math.log(6.0) - 3.4011974 * jax.random.uniform(key_list[7], (2, REC_KEYS), jnp.float32) ** block_levels(key_list[7], (2, REC_KEYS), ((1, 4),), -0.2, 0.2)), 0.2, 6.0)
    chain_gain = jnp.clip(1.0 + 0.18 * jax.random.normal(key_list[8], (REC_WIDTH,), jnp.float32), 0.1, 1.9)
    query_down = normal_values(key_list[9], (D, QLAT), D ** -0.5, 0.125, ((0, 64),))
    latent_down = normal_values(key_list[10], (D, KVLAT), D ** -0.5, 0.125, ((0, 64),))
    rotary_down = normal_values(key_list[11], (D, ROPE_DIM), D ** -0.5, 0.125)
    query_latent_gain = jnp.clip(1.0 + 0.18 * jax.random.normal(key_list[12], (QLAT,), jnp.float32), 0.1, 1.9)
    latent_gain = jnp.clip(1.0 + 0.18 * jax.random.normal(key_list[13], (KVLAT,), jnp.float32), 0.1, 1.9)
    query_up = normal_values(key_list[14], (QLAT, HEADS_ATT * ATT_QK), QLAT ** -0.5, 0.21875, ((1, 4),))
    latent_up = normal_values(key_list[15], (KVLAT, HEADS_ATT * (NOPE_DIM + VHEAD_DIM)), KVLAT ** -0.5, 0.25, ((1, 4),))
    query_head_gain = jnp.clip(1.0 + 0.18 * jax.random.normal(key_list[16], (ATT_QK,), jnp.float32), 0.1, 1.9)
    key_head_gain = jnp.clip(1.0 + 0.18 * jax.random.normal(key_list[17], (ATT_QK,), jnp.float32), 0.1, 1.9)
    mixer_gain = jnp.clip(1.0 + 0.18 * jax.random.normal(key_list[18], (ATT_WIDTH,), jnp.float32), 0.1, 1.9)
    chain_out = normal_values(key_list[19], (REC_WIDTH, D), (REC_WIDTH + ATT_WIDTH) ** -0.5, 0.125, ((0, 4), (1, 64)))
    attend_out = normal_values(key_list[20], (ATT_WIDTH, D), (REC_WIDTH + ATT_WIDTH) ** -0.5, 0.125, ((0, 4), (1, 64)))
    return dict(tokens=tokens, input_gain=input_gain, chain_query=chain_query, forward_gate=forward_gate, backward_gate=backward_gate, chain_value=chain_value, output_gate=output_gate, forget_rate=forget_rate, chain_gain=chain_gain, query_down=query_down, latent_down=latent_down, rotary_down=rotary_down, query_latent_gain=query_latent_gain, latent_gain=latent_gain, query_up=query_up, latent_up=latent_up, query_head_gain=query_head_gain, key_head_gain=key_head_gain, mixer_gain=mixer_gain, chain_out=chain_out, attend_out=attend_out)


norm_eps = 1e-06
rope_theta = 10000.0
finest_arithmetic_mode = lax.Precision.HIGHEST

def rms_scale(values, gain_vec):
    mean_square = lax.optimization_barrier(jnp.mean(values * values, axis=-1, keepdims=True))
    return values * lax.rsqrt(mean_square + norm_eps) * gain_vec

def rotate_tail(values, positions):
    half_dim = ROPE_DIM // 2
    inverse = rope_theta ** (-jnp.arange(0, ROPE_DIM, 2).astype(jnp.float32) / ROPE_DIM)
    angles = positions.astype(jnp.float32)[:, None] * inverse
    cosine = jnp.cos(angles)[:, None, :]
    sine_table = jnp.sin(angles)[:, None, :]
    unrotated = values[..., :NOPE_DIM]
    first_half = values[..., NOPE_DIM:NOPE_DIM + half_dim]
    latter_element = values[..., NOPE_DIM + half_dim:]
    return jnp.concatenate([unrotated, first_half * cosine - latter_element * sine_table, latter_element * cosine + first_half * sine_table], axis=-1)

def gate_parts(pre_gate, rate_row, seq_len):
    opening = rate_row / seq_len * jax.nn.sigmoid(-pre_gate.astype(jnp.float32))
    return (jnp.log1p(-opening), opening)

def summarize(query_rows, key_rows, payload_array_lines, log_decay):
    cumulative = jnp.cumsum(log_decay, axis=0)
    weighted_probe_vectors = query_rows * jnp.exp(cumulative)
    weighted_lookup_vectors = key_rows * jnp.exp(-cumulative)
    overall_shrink_multiplier = jnp.exp(cumulative[-1])
    recurrent_memory_digest = overall_shrink_multiplier[:, :, None] * jnp.einsum('jre,jrw->rew', weighted_lookup_vectors, payload_array_lines, precision=finest_arithmetic_mode)
    return (weighted_probe_vectors, weighted_lookup_vectors, overall_shrink_multiplier, recurrent_memory_digest)

def emit(weighted_probe_vectors, weighted_lookup_vectors, payload_array_lines, incoming_update):
    length = weighted_probe_vectors.shape[0]
    lower_mask = jnp.tril(jnp.ones((length, length), jnp.float32))
    scores = jnp.einsum('thk,shk->hts', weighted_probe_vectors, weighted_lookup_vectors, precision=finest_arithmetic_mode) * lower_mask
    within = jnp.einsum('hts,shv->thv', scores, payload_array_lines, precision=finest_arithmetic_mode)
    prior_state = jnp.einsum('mjf,jfi->mji', weighted_probe_vectors, incoming_update, precision=finest_arithmetic_mode)
    return within + prior_state

def run_chain(query_rows, key_rows, payload_array_lines, log_decay):
    seq_len, heads_here, key_dim = query_rows.shape
    blocks = seq_len // TOK_DEV

    def to_blocks(tensor):
        return tensor.reshape(blocks, TOK_DEV, heads_here, tensor.shape[2])

    def advance(carried, block_in):
        weighted_probe_vectors, weighted_lookup_vectors, overall_shrink_multiplier, recurrent_memory_digest = summarize(block_in[0], block_in[1], block_in[2], block_in[3])
        outputs = emit(weighted_probe_vectors, weighted_lookup_vectors, block_in[2], carried)
        return (overall_shrink_multiplier[:, :, None] * carried + recurrent_memory_digest, outputs)
    initial = jnp.zeros((heads_here, key_dim, payload_array_lines.shape[2]), jnp.float32)
    _, produced = lax.scan(advance, initial, (to_blocks(query_rows), to_blocks(key_rows), to_blocks(payload_array_lines), to_blocks(log_decay)))
    return produced.reshape(seq_len, heads_here, payload_array_lines.shape[2])

def reference(tokens, input_gain, chain_query, forward_gate, backward_gate, chain_value, output_gate, forget_rate, chain_gain, query_down, latent_down, rotary_down, query_latent_gain, latent_gain, query_up, latent_up, query_head_gain, key_head_gain, mixer_gain, chain_out, attend_out):
    seq_len = tokens.shape[0]
    normed = rms_scale(tokens.astype(jnp.float32), input_gain).astype(jnp.bfloat16)

    def project(source, weight):
        return jnp.dot(source, weight, preferred_element_type=jnp.float32).astype(jnp.bfloat16)

    def heads_of(tensor, head_width):
        return tensor.astype(jnp.float32).reshape(seq_len, tensor.shape[1] // head_width, head_width)
    query_rows = heads_of(project(normed, chain_query), KEY_DIM)
    payload_array_lines = heads_of(project(normed, chain_value), VAL_DIM)
    forward_log, forward_key = gate_parts(project(normed, forward_gate), forget_rate[0], seq_len)
    backward_log, backward_key = gate_parts(project(normed, backward_gate), forget_rate[1], seq_len)
    gate_logit = project(normed, output_gate).astype(jnp.float32)
    forward_out = run_chain(query_rows, heads_of(forward_key, KEY_DIM), payload_array_lines, heads_of(forward_log, KEY_DIM))
    reversed_out = run_chain(jnp.flip(query_rows, 0), jnp.flip(heads_of(backward_key, KEY_DIM), 0), jnp.flip(payload_array_lines, 0), jnp.flip(heads_of(backward_log, KEY_DIM), 0))
    combined = forward_out + jnp.flip(reversed_out, 0)
    head_gain = chain_gain.reshape(combined.shape[1], VAL_DIM)
    chain_mixed = (rms_scale(combined, head_gain).reshape(seq_len, -1) * jax.nn.silu(gate_logit)).astype(jnp.bfloat16)
    query_latent = rms_scale(project(normed, query_down).astype(jnp.float32), query_latent_gain).astype(jnp.bfloat16)
    pair_latent = rms_scale(project(normed, latent_down).astype(jnp.float32), latent_gain).astype(jnp.bfloat16)
    rotary_key = project(normed, rotary_down).astype(jnp.float32)
    attend_query = project(query_latent, query_up).astype(jnp.float32).reshape(seq_len, HEADS_ATT, ATT_QK)
    attend_pairs = project(pair_latent, latent_up).reshape(seq_len, HEADS_ATT, NOPE_DIM + VHEAD_DIM)
    positions = jnp.arange(seq_len, dtype=jnp.int32)
    query_final = rotate_tail(rms_scale(attend_query, query_head_gain), positions).astype(jnp.bfloat16)
    key_cat = jnp.concatenate([attend_pairs[..., :NOPE_DIM].astype(jnp.float32), jnp.broadcast_to(rotary_key[:, None, :], (seq_len, HEADS_ATT, ROPE_DIM))], axis=-1)
    key_final = rotate_tail(rms_scale(key_cat, key_head_gain), positions).astype(jnp.bfloat16)
    key_wide = key_final.astype(jnp.float32)
    value_wide = attend_pairs[..., NOPE_DIM:].astype(jnp.float32)
    score_scale = ATT_QK ** (-0.5)

    def attend(query_block):
        scores = jnp.einsum('qhd,khd->hqk', query_block.astype(jnp.float32), key_wide) * score_scale
        weights = jnp.exp(scores)
        rounded = lax.optimization_barrier(weights.astype(jnp.bfloat16)).astype(jnp.float32)
        numerator = jnp.einsum('hqk,khv->qhv', rounded, value_wide)
        return numerator / jnp.transpose(lax.optimization_barrier(jnp.sum(weights, axis=-1)))[:, :, None]
    blocks_in = query_final.reshape(seq_len // TOK_DEV, TOK_DEV, HEADS_ATT, ATT_QK)
    attend_rows = lax.map(attend, blocks_in).reshape(seq_len, HEADS_ATT, VHEAD_DIM)
    attend_mixed = rms_scale(attend_rows, mixer_gain.reshape(HEADS_ATT, VHEAD_DIM)).reshape(seq_len, ATT_WIDTH).astype(jnp.bfloat16)
    mixed_sum = jnp.dot(chain_mixed, chain_out, preferred_element_type=jnp.float32) + jnp.dot(attend_mixed, attend_out, preferred_element_type=jnp.float32)
    return mixed_sum
```

```python
import jax
import jax.numpy as jnp
from jax import lax
from jax.experimental import pallas as pl
from jax.experimental.pallas import tpu as pltpu
from jax.sharding import Mesh
from jax.sharding import PartitionSpec as P

HEAD = 128
NOPE = 128
ROPE = 64
QK = 192
QLAT = 768
KVLAT = 512
NZ, NY, NC, NX = 8, 4, 2, 4
EPS = 1e-06
THETA = 10000.0
SP = ("z", "y", "c")
F32 = jnp.float32
BF = jnp.bfloat16


def shift(value, axis, count, by):
    return lax.ppermute(value, axis, [(i, (i + by) % count) for i in range(count)])


def put(buffer, piece, index, axis):
    return lax.dynamic_update_slice_in_dim(buffer, piece, index, axis)


def direct(piece, axis, count):
    return [piece] + [shift(piece, axis, count, k) for k in range(1, count)]


def ring_z(piece):
    found = {0: piece}
    up = down = piece
    for k in range(1, 5):
        up = shift(up, "z", NZ, 1)
        found[k] = up
        if k < 4:
            down = shift(down, "z", NZ, -1)
            found[NZ - k] = down
    return [found[k] for k in range(NZ)]


def ordered(pieces, index, axis, shape, count):
    buffer = jnp.zeros(shape, pieces[0].dtype)
    for k, piece in enumerate(pieces):
        buffer = put(buffer, jnp.expand_dims(piece, axis), (index - k) % count, axis)
    return buffer


def y_then_z(piece, z, y):
    rows, cols = piece.shape
    slab = ordered(direct(piece, "y", NY), y, 0, (NY, rows, cols), NY).reshape(NY * rows, cols)
    full = ordered(ring_z(slab), z, 0, (NZ, NY * rows, cols), NZ)
    return full.reshape(NZ * NY * rows, cols)


def z_then_y(piece, z, y):
    rows, cols = piece.shape
    column = ordered(ring_z(piece), z, 0, (NZ, rows, cols), NZ)
    full = ordered(direct(column, "y", NY), y, 1, (NZ, NY, rows, cols), NY)
    return full.reshape(NZ * NY * rows, cols)


def core_pair(mine, theirs, c, axis):
    other = shift(theirs, "c", NC, 1)
    first = jnp.where(c == 0, mine, other)
    second = jnp.where(c == 0, other, mine)
    return jnp.concatenate([first, second], axis=axis)


def rms(values, gain):
    return values * lax.rsqrt(jnp.mean(values * values, axis=-1, keepdims=True) + EPS) * gain


def rotated(tail, cosine, sine):
    first, second = tail[:, : ROPE // 2], tail[:, ROPE // 2 :]
    return jnp.concatenate(
        [first * cosine - second * sine, second * cosine + first * sine], axis=-1
    )


def packed(tail):
    half = tail.shape[0] // 2
    return jnp.concatenate([tail[:half], tail[half:]], axis=1)


def attend_kernel(tokens, last, *refs):
    q_refs, kv_refs, rest = refs[:NY], refs[NY : NY + 2], refs[NY + 2 :]
    if len(rest) == 4:
        acc_ref, out_ref, key_scr, val_scr = rest
    else:
        acc_ref = None
        out_ref, key_scr, val_scr = rest
    half = tokens // 2
    for i, kv in enumerate(kv_refs):
        at = i * tokens
        key_scr[pl.ds(at, tokens), 0:128] = kv[0:tokens, :]
        tail = kv[2 * tokens : 2 * tokens + half, :]
        key_scr[pl.ds(at, half), 128:192] = tail[:, 0:64]
        key_scr[pl.ds(at + half, half), 128:192] = tail[:, 64:128]
        val_scr[pl.ds(at, tokens), 0:128] = kv[tokens : 2 * tokens, :]
    val_scr[:, 128:256] = jnp.ones((2 * tokens, 128), BF)
    factor = (QK**-0.5) * 1.4426950408889634
    keys = key_scr[...]
    values = val_scr[...]
    for i, q in enumerate(q_refs):
        for j in range(2):
            nope = q[pl.ds(j * half, half), :]
            tail = q[tokens : tokens + half, 64 * j : 64 * j + 64]
            query = jnp.concatenate([nope, tail], axis=1)
            scores = lax.dot_general(
                query, keys, (((1,), (1,)), ((), ())), preferred_element_type=F32
            )
            weights = jnp.exp2(scores * factor).astype(BF)
            sums = jnp.dot(weights, values, preferred_element_type=F32)
            at = pl.ds(i * tokens + j * half, half)
            if acc_ref is not None:
                sums = sums + acc_ref[at, :]
            if last:
                out_ref[at, 0:128] = sums[:, 0:128].astype(BF)
                den = sums[:, 128:256]
                high = den.astype(BF)
                low = (den - high.astype(F32)).astype(BF)
                lane = lax.broadcasted_iota(jnp.int32, (half, 128), 1)
                out_ref[at, 128:256] = jnp.where(lane < 64, high, low)
            else:
                out_ref[at, :] = sums


def attend(queries, pair, acc, last):
    tokens = pair[0].shape[0] * 2 // 5
    rows = NY * tokens
    args = list(queries) + list(pair) + ([] if acc is None else [acc])
    flops = 2 * rows * 2 * tokens * 512

    def body(*refs):
        attend_kernel(tokens, last, *refs)

    return pl.pallas_call(
        body,
        out_shape=jax.ShapeDtypeStruct((rows, 256), BF if last else F32),
        in_specs=[pl.BlockSpec(memory_space=pltpu.VMEM)] * len(args),
        out_specs=pl.BlockSpec(memory_space=pltpu.VMEM),
        scratch_shapes=[
            pltpu.VMEM((2 * tokens, QK), BF),
            pltpu.VMEM((2 * tokens, 256), BF),
        ],
        cost_estimate=pl.CostEstimate(
            flops=flops, bytes_accessed=4 * rows * 256, transcendentals=rows * 2 * tokens
        ),
        name="attend",
    )(*args)


def on_device(
    tokens,
    input_gain,
    chain_query,
    forward_gate,
    backward_gate,
    chain_value,
    output_gate,
    forget_rate,
    chain_gain,
    query_down,
    latent_down,
    rotary_down,
    query_latent_gain,
    latent_gain,
    query_up,
    latent_up,
    query_head_gain,
    key_head_gain,
    mixer_gain,
    chain_out,
    attend_out,
):
    z, y, c, x = (lax.axis_index(a) for a in ("z", "y", "c", "x"))
    rows = tokens.shape[0]
    block = rows * NC
    seq_len = block * NY * NZ

    def half_cols(weight, which, width):
        return lax.dynamic_slice_in_dim(weight, which * width, width, 1)

    def low_cols(which):
        eighth = x * NC + which
        return [
            half_cols(query_down, eighth, QLAT // 8),
            half_cols(latent_down, eighth, KVLAT // 8),
        ]

    def group_a(which):
        return jnp.concatenate(
            [half_cols(w, which, HEAD) for w in (chain_query, forward_gate, backward_gate)], axis=1
        )

    def group_b(which):
        pad = jnp.zeros((query_down.shape[0], 96), BF)
        return jnp.concatenate(
            [half_cols(w, which, HEAD) for w in (chain_value, output_gate)]
            + low_cols(which)
            + [pad],
            axis=1,
        )

    def out_rows(which):
        both = [
            lax.dynamic_slice_in_dim(w, which * HEAD, HEAD, 0) for w in (chain_out, attend_out)
        ]
        return jnp.concatenate(both, axis=0).T

    token_block = core_pair(tokens, tokens, c, 0)
    piece_b = core_pair(group_b(c), group_b(1 - c), c, 0)
    piece_a = core_pair(group_a(c), group_a(1 - c), c, 0)
    weight_b = z_then_y(piece_b, z, y)
    weight_a = y_then_z(piece_a, z, y)
    normed = rms(token_block.astype(F32), input_gain).astype(BF)

    def project(source, weight):
        return jnp.dot(source, weight, preferred_element_type=F32).astype(BF)

    made_b = project(normed, weight_b)
    rotary_key = project(normed, rotary_down).astype(F32)
    low = made_b[:, 256:512]

    by_x = direct(low, "x", NX)
    both = [(piece, shift(piece, "c", NC, 1)) for piece in by_x]
    q_low = jnp.zeros((block, 8, QLAT // 8), BF)
    kv_low = jnp.zeros((block, 8, KVLAT // 8), BF)
    for k, pair in enumerate(both):
        for who, piece in enumerate(pair):
            at = ((x - k) % NX) * NC + (c if who == 0 else 1 - c)
            q_low = put(q_low, piece[:, None, : QLAT // 8], at, 1)
            kv_low = put(kv_low, piece[:, None, QLAT // 8 : (QLAT + KVLAT) // 8], at, 1)
    query_latent = rms(q_low.reshape(block, QLAT).astype(F32), query_latent_gain).astype(BF)
    pair_latent = rms(kv_low.reshape(block, KVLAT).astype(F32), latent_gain).astype(BF)

    attend_query = project(query_latent, half_cols(query_up, c, QK)).astype(F32)
    attend_pairs = project(pair_latent, half_cols(latent_up, c, 2 * HEAD))
    positions = ((z * NY + y) * block + jnp.arange(block, dtype=jnp.int32)).astype(F32)
    inverse = THETA ** (-jnp.arange(0, ROPE, 2).astype(F32) / ROPE)
    angles = positions[:, None] * inverse
    cosine, sine = jnp.cos(angles), jnp.sin(angles)
    query_scaled = rms(attend_query, query_head_gain)
    key_scaled = rms(
        jnp.concatenate([attend_pairs[:, :NOPE].astype(F32), rotary_key], axis=1), key_head_gain
    )
    query_piece = jnp.concatenate(
        [
            query_scaled[:, :NOPE].astype(BF),
            packed(rotated(query_scaled[:, NOPE:], cosine, sine).astype(BF)),
        ],
        axis=0,
    )
    kv_piece = jnp.concatenate(
        [
            key_scaled[:, :NOPE].astype(BF),
            attend_pairs[:, NOPE:],
            packed(rotated(key_scaled[:, NOPE:], cosine, sine).astype(BF)),
        ],
        axis=0,
    )
    queries = direct(query_piece, "y", NY)
    kv = ring_z(kv_piece)
    acc = attend(queries, (kv[1], kv[7]), None, False)
    acc = attend(queries, (kv[2], kv[6]), acc, False)
    acc = attend(queries, (kv[3], kv[5]), acc, False)
    part = attend(queries, (kv[4], kv[0]), acc, True)

    made_a = project(normed, weight_a)
    chain_q = made_a[:, :HEAD].astype(F32)
    payload = made_b[:, :HEAD]
    gate_logit = made_b[:, HEAD : 2 * HEAD].astype(F32)
    rates = lax.dynamic_slice_in_dim(forget_rate, c * HEAD, HEAD, 1) / seq_len
    key_f = rates[0] * jax.nn.sigmoid(-made_a[:, HEAD : 2 * HEAD].astype(F32))
    key_b = rates[1] * jax.nn.sigmoid(-made_a[:, 2 * HEAD :].astype(F32))
    row_at = lax.broadcasted_iota(jnp.int32, (block, block), 0)
    col_at = lax.broadcasted_iota(jnp.int32, (block, block), 1)
    lower = (row_at >= col_at).astype(F32)
    upper = (row_at <= col_at).astype(F32)
    cum_f = jnp.dot(lower, jnp.log1p(-key_f), precision=lax.Precision.HIGHEST)
    cum_b = jnp.dot(upper, jnp.log1p(-key_b), precision=lax.Precision.HIGHEST)
    probe_f = (chain_q * jnp.exp(cum_f)).astype(BF)
    probe_b = (chain_q * jnp.exp(cum_b)).astype(BF)
    look_f = (key_f * jnp.exp(-cum_f)).astype(BF)
    look_b = (key_b * jnp.exp(-cum_b)).astype(BF)

    def contract(a, b, dims):
        return lax.dot_general(a, b, (dims, ((), ())), preferred_element_type=F32)

    within = lower * contract(probe_f, look_f, ((1,), (1,))) + upper * contract(
        probe_b, look_b, ((1,), (1,))
    )
    inside = jnp.dot(within.astype(BF), payload, preferred_element_type=F32)
    total_f, total_b = cum_f[-1], cum_b[0]
    digest_f = jnp.exp(total_f)[:, None] * contract(look_f, payload, ((0,), (0,)))
    digest_b = jnp.exp(total_b)[:, None] * contract(look_b, payload, ((0,), (0,)))

    def with_logs(digests, logs):
        rows_out = []
        for log in logs:
            high = log.astype(BF)
            rows_out += [high, (log - high.astype(F32)).astype(BF)]
        rows_out += [jnp.zeros_like(rows_out[0])] * (16 - len(rows_out))
        return jnp.concatenate([d.astype(BF) for d in digests] + [jnp.stack(rows_out)], axis=0)

    packet = with_logs((digest_f, digest_b), (total_f, total_b))
    slab = lax.all_to_all(
        jnp.broadcast_to(packet, (NY,) + packet.shape), "y", 0, 0, tiled=True
    ).astype(F32)
    slab_f, slab_b, slab_log = slab[:, :HEAD], slab[:, HEAD : 2 * HEAD], slab[:, 2 * HEAD :]
    log_f = slab_log[:, 0] + slab_log[:, 1]
    log_b = slab_log[:, 2] + slab_log[:, 3]

    def carried(states, logs, position, order, before):
        state = jnp.zeros((HEAD, HEAD), F32)
        log = jnp.zeros((HEAD,), F32)
        for j in order:
            new_state = jnp.exp(logs[j])[:, None] * state + states[j]
            passed = before(j, position)
            state = jnp.where(passed, new_state, state)
            log = jnp.where(passed, log + logs[j], log)
        return state, log

    def earlier(j, position):
        return j < position

    def later(j, position):
        return j > position

    def always(j, position):
        return True

    up_y, down_y = range(NY), range(NY - 1, -1, -1)
    all_f, all_log_f = carried(slab_f, log_f, y, up_y, always)
    all_b, all_log_b = carried(slab_b, log_b, y, down_y, always)
    in_f, in_log_f = carried(slab_f, log_f, y, up_y, earlier)
    in_b, in_log_b = carried(slab_b, log_b, y, down_y, later)
    send_f = with_logs((all_f,), (all_log_f,))
    send_b = with_logs((all_b,), (all_log_b,))
    to = lax.broadcasted_iota(jnp.int32, (NZ, 1, 1), 0)
    outer = lax.all_to_all(
        jnp.where(to > z, send_f[None], send_b[None]), "z", 0, 0, tiled=True
    ).astype(F32)
    outer_log = outer[:, HEAD] + outer[:, HEAD + 1]
    far_f, _ = carried(outer[:, :HEAD], outer_log, z, range(NZ), earlier)
    far_b, _ = carried(outer[:, :HEAD], outer_log, z, range(NZ - 1, -1, -1), later)
    state_f = in_f + jnp.exp(in_log_f)[:, None] * far_f
    state_b = in_b + jnp.exp(in_log_b)[:, None] * far_b
    combined = (
        inside
        + jnp.dot(probe_f, state_f.astype(BF), preferred_element_type=F32)
        + jnp.dot(probe_b, state_b.astype(BF), preferred_element_type=F32)
    )
    head_gain = lax.dynamic_slice_in_dim(chain_gain, c * HEAD, HEAD, 0)
    chain_mixed = (rms(combined, head_gain) * jax.nn.silu(gate_logit)).astype(BF)

    piece_o = core_pair(out_rows(c), out_rows(1 - c), c, 0)
    piece_o, _ = lax.optimization_barrier((piece_o, made_b))
    weight_o = y_then_z(piece_o, z, y)

    sums = part[:block].astype(F32)
    for k in range(1, NY):
        sums = sums + shift(part[k * block : (k + 1) * block], "y", NY, -k).astype(F32)
    attend_rows = sums[:, :HEAD] / (sums[:, HEAD : HEAD + 1] + sums[:, HEAD + 64 : HEAD + 65])
    attend_gain = lax.dynamic_slice_in_dim(mixer_gain, c * HEAD, HEAD, 0)
    attend_mixed = rms(attend_rows, attend_gain).astype(BF)
    mixed = jnp.concatenate([chain_mixed, attend_mixed], axis=1)
    partial = contract(mixed, weight_o, ((1,), (1,)))
    mine = lax.dynamic_slice_in_dim(partial, c * rows, rows, 0)
    theirs = lax.dynamic_slice_in_dim(partial, (1 - c) * rows, rows, 0).astype(BF)
    summed = mine + shift(theirs, "c", NC, 1).astype(F32)
    quarter = rows // NX

    def quarter_of(which):
        return lax.dynamic_slice_in_dim(summed, (which % NX) * quarter, quarter, 0)

    result = quarter_of(x)
    for k in range(1, NX):
        result = result + shift(quarter_of(x + k).astype(BF), "x", NX, k).astype(F32)
    return result


def solution(mesh):
    torus = Mesh(mesh.devices.reshape(NZ, NY, NC, NX), ("z", "y", "c", "x"))
    placed = (
        P(SP, None),
        P(),
        P(SP, "x"),
        P(SP, "x"),
        P(SP, "x"),
        P(SP, "x"),
        P(SP, "x"),
        P(None, "x"),
        P("x"),
        P(SP, None),
        P(SP, None),
        P(),
        P(),
        P(),
        P(None, "x"),
        P(None, "x"),
        P(),
        P(),
        P("x"),
        P("x", SP),
        P("x", SP),
    )
    return jax.shard_map(
        on_device, mesh=torus, in_specs=placed, out_specs=P(SP + ("x",), None), check_vma=False
    )
```

```python
import jax
import jax.numpy as jnp
from jax import lax
from jax.experimental import pallas as pl
from jax.experimental.pallas import tpu as pltpu
from jax.sharding import Mesh
from jax.sharding import PartitionSpec as P

HEAD = 128
ROPE = 64
QK = 192
QLAT = 768
KVLAT = 512
Q8 = QLAT // 8
KV8 = KVLAT // 8
NZ, NY, NC, NX = 8, 4, 2, 4
EPS = 1e-06
THETA = 10000.0
SP = ("z", "y", "c")
F32 = jnp.float32
BF = jnp.bfloat16
LOG2E = 1.4426950408889634


def shift(value, axis, count, by):
    return lax.ppermute(value, axis, [(i, (i + by) % count) for i in range(count)])


def exchange(value, axis):
    return lax.all_to_all(value, axis, 0, 0, tiled=True)


def ring_z(piece):
    found = {0: piece}
    up = down = piece
    for k in range(1, 5):
        up = shift(up, "z", NZ, 1)
        found[k] = up
        if k < 4:
            down = shift(down, "z", NZ, -1)
            found[NZ - k] = down
    return [found[k] for k in range(NZ)]


def dot(a, b):
    return lax.dot_general(a, b, (((1,), (0,)), ((), ())), preferred_element_type=F32)


def dot_nt(a, b):
    return lax.dot_general(a, b, (((1,), (1,)), ((), ())), preferred_element_type=F32)


def dot_tn(a, b):
    return lax.dot_general(a, b, (((0,), (0,)), ((), ())), preferred_element_type=F32)


def inverse_rms(square_sum, width):
    return lax.rsqrt(square_sum * (1.0 / width) + EPS)


def squares(values):
    return jnp.sum(values * values, axis=-1, keepdims=True)


def call(body, outs, scalars, args, name, scratch=(), specs=None, flops=1 << 20, grid=()):
    whole = pl.BlockSpec(memory_space=pltpu.VMEM)
    in_specs = [pl.BlockSpec(memory_space=pltpu.SMEM)] + [
        whole if specs is None or specs[i] is None else specs[i] for i in range(len(args))
    ]
    single = not isinstance(outs, list)
    return pl.pallas_call(
        body,
        out_shape=outs,
        grid=grid,
        in_specs=in_specs,
        out_specs=whole if single else [whole] * len(outs),
        scratch_shapes=list(scratch),
        cost_estimate=pl.CostEstimate(flops=flops, bytes_accessed=1 << 20, transcendentals=0),
        name=name,
    )(scalars, *args)


def made(shape, dtype):
    return jax.ShapeDtypeStruct(shape, dtype)


def prep_kernel(where, cq, fg, bg, cv, og, qd, ld, co, ao, out_a, out_b):
    x = where[3]
    n = cq.shape[0]
    row = lax.broadcasted_iota(jnp.int32, (n, n), 0)
    eye = (row == lax.broadcasted_iota(jnp.int32, (n, n), 1)).astype(BF)
    for j in range(NC):
        lanes = slice(j * HEAD, (j + 1) * HEAD)
        wide = [dot_nt(eye, co[lanes, :]).astype(BF), dot_nt(eye, ao[lanes, :]).astype(BF)]
        wide += [w[:, lanes] for w in (cq, fg, bg, cv, og)]
        for k in range(NY):
            for i, value in enumerate(wide):
                out_a[k, j, :, i * HEAD : (i + 1) * HEAD] = value
        out_b[0, j, :, :] = jnp.zeros((n, 256), BF)
        for i in range(NX):

            @pl.when(x == i)
            def _():
                e = i * NC + j
                out_b[0, j, :, 0:Q8] = qd[:, e * Q8 : (e + 1) * Q8]
                out_b[0, j, :, HEAD : HEAD + KV8] = ld[:, e * KV8 : (e + 1) * KV8]

        ready = out_b[0, j, :, :]
        for k in range(1, NZ):
            out_b[k, j, :, :] = ready


def low_kernel(where, mine, other, gain, b0, b1, b2, b3, rot, normed, low, rotary, w_scr):
    y, c = where[1], where[2]
    half = mine.shape[0]
    for ref, at in ((mine, c), (other, 1 - c)):
        values = ref[...].astype(F32)
        values = values * inverse_rms(squares(values), values.shape[1]) * gain[...]
        normed[pl.ds(pl.multiple_of(at * half, half), half), :] = values.astype(BF)
    for k, ref in enumerate((b0, b1, b2, b3)):
        which = lax.rem(y - k + NY, NY)
        for i in range(NZ):
            at = pl.multiple_of((i * NY + which) * 64, 64)
            w_scr[pl.ds(at, 64), :] = ref[i]
    ready = dot(normed[...], w_scr[...]).astype(BF)
    for k in range(NX):
        low[k] = ready
    rotary[...] = dot(normed[...], rot[...]).astype(BF)


def chain_kernel(where, rates, normed, *refs):
    pieces, (inside, probe_f, probe_b, gate, packet) = refs[:NZ], refs[NZ:]
    z = where[0]
    acc = None
    for k, ref in enumerate(pieces):
        at = pl.multiple_of(lax.rem(z - k + NZ, NZ) * 256, 256)
        part = dot(normed[:, pl.ds(at, 256)], ref[:, 256:896])
        acc = part if acc is None else acc + part
    ready = acc.astype(BF)
    n = ready.shape[0]
    query = ready[:, 0:128].astype(F32)
    payload = ready[:, 384:512]
    gate[...] = ready[:, 512:640]
    row = lax.broadcasted_iota(jnp.int32, (n, n), 0)
    col = lax.broadcasted_iota(jnp.int32, (n, n), 1)
    within = None
    logs = []
    for d in range(2):
        keep = (row >= col) if d == 0 else (row <= col)
        logit = ready[:, 128 * (d + 1) : 128 * (d + 2)].astype(F32)
        key = rates[d : d + 1, :] * jax.nn.sigmoid(-logit)
        log = jnp.log1p(-key)
        high = log.astype(BF)
        rest = (log - high.astype(F32)).astype(BF)
        tri = keep.astype(BF)
        cum = dot(tri, high) + dot(tri, rest)
        total = cum[n - 1 : n, :] if d == 0 else cum[0:1, :]
        probe = (query * jnp.exp(cum)).astype(BF)
        look = (key * jnp.exp(-cum)).astype(BF)
        (probe_f if d == 0 else probe_b)[...] = probe
        score = jnp.where(keep, dot_nt(probe, look), 0.0)
        within = score if within is None else within + score
        digest = dot_tn(payload, (key * jnp.exp(total - cum)).astype(BF)).astype(BF)
        for k in range(NY):
            packet[k, d * HEAD : (d + 1) * HEAD, :] = digest
        high = total.astype(BF).astype(F32)
        logs += [high, total - high]
    inside[...] = dot(within.astype(BF), payload)
    at = lax.broadcasted_iota(jnp.int32, (16, HEAD), 0)
    tail = jnp.zeros((16, HEAD), F32)
    for i, log in enumerate(logs):
        tail = jnp.where(at == i, log, tail)
    tail = tail.astype(BF)
    for k in range(NY):
        packet[k, 2 * HEAD : 2 * HEAD + 16, :] = tail


def walk(states, logs, order, chosen):
    state = jnp.zeros((HEAD, HEAD), F32)
    log = jnp.zeros((1, HEAD), F32)
    for j in order:
        fresh = state * jnp.exp(logs(j)) + states(j)
        passed = chosen(j)
        state = jnp.where(passed, fresh, state)
        log = jnp.where(passed, log + logs(j), log)
    return state, log


def slab_kernel(where, slab, state_f, state_b, log_out, send):
    z, y = where[0], where[1]
    at = lax.broadcasted_iota(jnp.int32, (16, HEAD), 0)
    kept = []
    for d in range(2):
        order = range(NY) if d == 0 else range(NY - 1, -1, -1)

        def states(j):
            return slab[j, d * HEAD : (d + 1) * HEAD, :].astype(F32)

        def logs(j):
            block = slab[j, 2 * HEAD : 2 * HEAD + 16, :].astype(F32)
            return block[2 * d : 2 * d + 1, :] + block[2 * d + 1 : 2 * d + 2, :]

        part, log = walk(states, logs, order, (lambda j: j < y) if d == 0 else (lambda j: j > y))
        full, full_log = walk(states, logs, order, lambda j: j >= 0)
        (state_f if d == 0 else state_b)[...] = part
        log_out[d : d + 1, :] = log
        high = full_log.astype(BF).astype(F32)
        tail = jnp.where(at == 0, high, jnp.where(at == 1, full_log - high, 0.0)).astype(BF)
        kept.append((full.astype(BF), tail))
    for k in range(NZ):
        ahead = k > z
        send[k, 0:HEAD, :] = jnp.where(ahead, kept[0][0], kept[1][0])
        send[k, HEAD : HEAD + 16, :] = jnp.where(ahead, kept[0][1], kept[1][1])


def close_kernel(
    where, outer, state_f, state_b, log_in, probe_f, probe_b, inside, gate, gain, mixed
):
    z = where[0]
    combined = inside[...]
    for d in range(2):
        order = range(NZ) if d == 0 else range(NZ - 1, -1, -1)

        def states(j):
            return outer[j, 0:HEAD, :].astype(F32)

        def logs(j):
            block = outer[j, HEAD : HEAD + 16, :].astype(F32)
            return block[0:1, :] + block[1:2, :]

        far, _ = walk(states, logs, order, (lambda j: j < z) if d == 0 else (lambda j: j > z))
        near = (state_f if d == 0 else state_b)[...]
        state = near + far * jnp.exp(log_in[d : d + 1, :])
        probe = (probe_f if d == 0 else probe_b)[...]
        combined = combined + dot_nt(probe, state.astype(BF))
    opened = gate[...].astype(F32)
    opened = opened * jax.nn.sigmoid(opened)
    scale = inverse_rms(squares(combined), HEAD)
    mixed[...] = (combined * scale * gain[...] * opened).astype(BF)


def heads_kernel(
    where, own, oth, q_up, kv_up, q_gain, kv_gain, rotary, cos, sin, qh_gain, kh_gain, q_out, kv_out
):
    c = where[2]
    n = rotary.shape[0]
    half = n // 2
    blocks = [(own, k, k * NC + c) for k in range(NX)] + [
        (oth, k, k * NC + 1 - c) for k in range(NX)
    ]

    def latent(first, width, up, gain):
        total = None
        for ref, k, _ in blocks:
            part = squares(ref[k, :, first : first + width].astype(F32))
            total = part if total is None else total + part
        scale = inverse_rms(total, width * 8)
        acc = None
        for ref, k, e in blocks:
            values = ref[k, :, first : first + width].astype(F32)
            values = (values * scale * gain[pl.ds(e, 1), :]).astype(BF)
            part = dot(values, up[pl.ds(pl.multiple_of(e * width, 32), width), :])
            acc = part if acc is None else acc + part
        return acc.astype(BF)

    query = latent(0, Q8, q_up, q_gain).astype(F32)
    pairs = latent(HEAD, KV8, kv_up, kv_gain)

    def turned(tail):
        swapped = jnp.concatenate([tail[:, ROPE // 2 :], tail[:, : ROPE // 2]], axis=1)
        return (tail * cos[...] + swapped * sin[...]).astype(BF)

    scale = inverse_rms(squares(query), QK)
    query = query * scale * qh_gain[...]
    nope = query[:, 0:HEAD].astype(BF)
    tail = turned(query[:, HEAD:QK])
    for k in range(NY):
        q_out[k, 0:n, :] = nope
        q_out[k, n : n + half, 0:ROPE] = tail[0:half]
        q_out[k, n : n + half, ROPE:HEAD] = tail[half:n]
    key = pairs[:, 0:HEAD].astype(F32)
    rope = rotary[...].astype(F32)
    scale = inverse_rms(squares(key) + squares(rope), QK)
    kv_out[0:n, :] = (key * scale * kh_gain[:, 0:HEAD]).astype(BF)
    kv_out[n : 2 * n, :] = pairs[:, HEAD : 2 * HEAD]
    tail = turned(rope * scale * kh_gain[:, HEAD:QK])
    kv_out[2 * n : 2 * n + half, 0:ROPE] = tail[0:half]
    kv_out[2 * n : 2 * n + half, ROPE:HEAD] = tail[half:n]


def attend_kernel(count, last, where, queries, *refs):
    kv_refs, rest = refs[:count], refs[count:]
    acc_ref = rest[0] if len(rest) == 5 else None
    out, q_scr, key_scr, val_scr = rest[-4:]
    n = queries.shape[1] * 2 // 3
    half = n // 2
    for i, kv in enumerate(kv_refs):
        at = i * n
        key_scr[at : at + n, 0:HEAD] = kv[0:n, :]
        tail = kv[2 * n : 2 * n + half, :]
        key_scr[at : at + half, HEAD:QK] = tail[:, 0:ROPE]
        key_scr[at + half : at + n, HEAD:QK] = tail[:, ROPE:HEAD]
        val_scr[at : at + n, 0:HEAD] = kv[n : 2 * n, :]
    val_scr[:, HEAD : 2 * HEAD] = jnp.ones((count * n, HEAD), BF)
    for i in range(NY):
        q_scr[0:n, 0:HEAD] = queries[i, 0:n, :]
        tail = queries[i, n : n + half, :]
        q_scr[0:half, HEAD:QK] = tail[:, 0:ROPE]
        q_scr[half:n, HEAD:QK] = tail[:, ROPE:HEAD]
        scores = dot_nt(q_scr[...], key_scr[...])
        weights = jnp.exp2(scores * (QK**-0.5 * LOG2E)).astype(BF)
        sums = dot(weights, val_scr[...])
        if acc_ref is not None:
            sums = sums + acc_ref[i]
        if last:
            out[i, :, 0:HEAD] = sums[:, 0:HEAD].astype(BF)
            den = sums[:, HEAD : 2 * HEAD]
            high = den.astype(BF)
            low = (den - high.astype(F32)).astype(BF)
            lane = lax.broadcasted_iota(jnp.int32, (n, HEAD), 1)
            out[i, :, HEAD : 2 * HEAD] = jnp.where(lane < ROPE, high, low)
        else:
            out[i] = sums


def attend(scalars, queries, pieces, acc, last):
    n = pieces[0].shape[0] * 2 // 5
    args = [queries] + list(pieces) + ([] if acc is None else [acc])
    count = len(pieces)

    def body(*refs):
        attend_kernel(count, last, *refs)

    return call(
        body,
        made((NY, n, 2 * HEAD), BF if last else F32),
        scalars,
        args,
        "attend",
        scratch=[
            pltpu.VMEM((n, QK), BF),
            pltpu.VMEM((count * n, QK), BF),
            pltpu.VMEM((count * n, 2 * HEAD), BF),
        ],
        flops=2 * NY * n * count * n * 512,
    )


def final_kernel(where, parts, chain, gain, *refs):
    pieces, (mine, theirs, scr) = refs[:NZ], refs[NZ:]
    z, c = where[0], where[2]
    n = chain.shape[0]
    half = n // 2
    sums = parts[0].astype(F32)
    for k in range(1, NY):
        sums = sums + parts[k].astype(F32)
    den = sums[:, HEAD : HEAD + 1] + sums[:, HEAD + ROPE : HEAD + ROPE + 1]
    rows = sums[:, 0:HEAD] / den
    scale = inverse_rms(squares(rows), HEAD)
    scr[:, 0:HEAD] = chain[...]
    scr[:, HEAD : 2 * HEAD] = (rows * scale * gain[...]).astype(BF)
    first = scr[pl.ds(pl.multiple_of(c * half, half), half), :]
    second = scr[pl.ds(pl.multiple_of((1 - c) * half, half), half), :]
    for k, ref in enumerate(pieces):
        at = pl.ds(pl.multiple_of(lax.rem(z - k + NZ, NZ) * 256, 256), 256)
        weight = ref[...]
        mine[:, at] = dot_nt(first, weight)
        theirs[:, at] = dot_nt(second, weight).astype(BF)


def on_device(
    tokens,
    input_gain,
    chain_query,
    forward_gate,
    backward_gate,
    chain_value,
    output_gate,
    forget_rate,
    chain_gain,
    query_down,
    latent_down,
    rotary_down,
    query_latent_gain,
    latent_gain,
    query_up,
    latent_up,
    query_head_gain,
    key_head_gain,
    mixer_gain,
    chain_out,
    attend_out,
):
    z, y, c, x = (lax.axis_index(a) for a in ("z", "y", "c", "x"))
    where = jnp.stack([z, y, c, x]).astype(jnp.int32)
    rows, width = tokens.shape
    n = rows * NC
    seq_len = n * NY * NZ
    piece = chain_query.shape[0]

    def cols(weight, size):
        return lax.dynamic_slice_in_dim(weight, c * size, size, 1)

    send_a, send_b = call(
        prep_kernel,
        [made((NY, NC, piece, 896), BF), made((NZ, NC, piece, 256), BF)],
        where,
        (
            chain_query,
            forward_gate,
            backward_gate,
            chain_value,
            output_gate,
            query_down,
            latent_down,
            chain_out,
            attend_out,
        ),
        "prep",
    )
    other = shift(tokens, "c", NC, 1)
    column = exchange(send_b.reshape(NZ * NC, piece, 256), ("z", "c")).reshape(NZ, NC * piece, 256)
    slab_a = exchange(send_a.reshape(NY * NC, piece, 896), ("y", "c")).reshape(-1, 896)
    columns = [column] + [shift(column, "y", NY, k) for k in range(1, NY)]
    ring_a = ring_z(slab_a)

    normed, low, rotary = call(
        low_kernel,
        [made((n, width), BF), made((NX, n, 256), BF), made((n, ROPE), BF)],
        where,
        [tokens, other, input_gain[None]] + columns + [rotary_down],
        "low",
        scratch=[pltpu.VMEM((width, 256), BF)],
        flops=2 * n * width * 320,
    )
    by_x = exchange(low, "x")
    by_x_other = shift(by_x, "c", NC, 1)
    positions = ((z * NY + y) * n + jnp.arange(n, dtype=jnp.int32)).astype(F32)
    inverse = THETA ** (-jnp.arange(0, ROPE, 2).astype(F32) / ROPE)
    angles = positions[:, None] * inverse
    cosine, sine = jnp.cos(angles), jnp.sin(angles)
    queries, kv_piece = call(
        heads_kernel,
        [made((NY, n * 3 // 2, HEAD), BF), made((n * 5 // 2, HEAD), BF)],
        where,
        (
            by_x,
            by_x_other,
            cols(query_up, QK),
            cols(latent_up, 2 * HEAD),
            query_latent_gain.reshape(8, Q8),
            latent_gain.reshape(8, KV8),
            rotary,
            jnp.concatenate([cosine, cosine], axis=1),
            jnp.concatenate([-sine, sine], axis=1),
            query_head_gain[None],
            key_head_gain[None],
        ),
        "heads",
        flops=2 * n * (QLAT * QK + KVLAT * 256),
    )
    queries = exchange(queries, "y")
    kv = ring_z(kv_piece)
    acc = attend(where, queries, [kv[k] for k in (0, 1, 7, 2, 6)], None, False)
    part = attend(where, queries, [kv[k] for k in (3, 5, 4)], acc, True)
    parts = exchange(part, "y")

    inside, probe_f, probe_b, gate, packet = call(
        chain_kernel,
        [
            made((n, HEAD), F32),
            made((n, HEAD), BF),
            made((n, HEAD), BF),
            made((n, HEAD), BF),
            made((NY, 2 * HEAD + 16, HEAD), BF),
        ],
        where,
        [cols(forget_rate, HEAD) / seq_len, normed] + ring_a,
        "chain",
        flops=2 * n * width * 640,
    )
    slab = exchange(packet, "y")
    state_f, state_b, log_in, send = call(
        slab_kernel,
        [
            made((HEAD, HEAD), F32),
            made((HEAD, HEAD), F32),
            made((2, HEAD), F32),
            made((NZ, HEAD + 16, HEAD), BF),
        ],
        where,
        (slab,),
        "slab",
    )
    outer = exchange(send, "z")

    def head_gain(gain):
        return lax.dynamic_slice_in_dim(gain[None], c * HEAD, HEAD, 1)

    chain_mixed = call(
        close_kernel,
        made((n, HEAD), BF),
        where,
        (
            outer,
            state_f,
            state_b,
            log_in,
            probe_f,
            probe_b,
            inside,
            gate,
            head_gain(chain_gain),
        ),
        "close",
    )
    whole = pl.BlockSpec(memory_space=pltpu.VMEM)
    out_block = pl.BlockSpec((256, 256), lambda i: (0, 0))
    mine, theirs = call(
        final_kernel,
        [made((rows, width), F32), made((rows, width), BF)],
        where,
        [parts, chain_mixed, head_gain(mixer_gain)] + ring_a,
        "final",
        scratch=[pltpu.VMEM((n, 2 * HEAD), BF)],
        specs=[whole] * 3 + [out_block] * NZ,
        flops=2 * n * width * 256,
        grid=(1,),
    )
    summed = (mine + shift(theirs, "c", NC, 1).astype(F32)).astype(BF)
    received = exchange(summed.reshape(NX, rows // NX, width), "x")
    return jnp.sum(received.astype(F32), axis=0)


def solution(mesh):
    torus = Mesh(mesh.devices.reshape(NZ, NY, NC, NX), ("z", "y", "c", "x"))
    placed = (
        P(SP, None),
        P(),
        P(SP, "x"),
        P(SP, "x"),
        P(SP, "x"),
        P(SP, "x"),
        P(SP, "x"),
        P(None, "x"),
        P("x"),
        P(SP, None),
        P(SP, None),
        P(),
        P(),
        P(),
        P(None, "x"),
        P(None, "x"),
        P(),
        P(),
        P("x"),
        P("x", SP),
        P("x", SP),
    )
    return jax.shard_map(
        on_device, mesh=torus, in_specs=placed, out_specs=P(SP + ("x",), None), check_vma=False
    )
```

```python
import jax
import jax.numpy as jnp
from jax import lax
from jax.experimental import pallas as pl
from jax.experimental.pallas import tpu as pltpu
from jax.sharding import Mesh
from jax.sharding import PartitionSpec as P

HEAD = 128
ROPE = 64
QK = 192
QLAT = 768
KVLAT = 512
Q8 = QLAT // 8
KV8 = KVLAT // 8
NZ, NY, NC, NX = 8, 4, 2, 4
EPS = 1e-06
THETA = 10000.0
SP = ("z", "y", "c")
F32 = jnp.float32
BF = jnp.bfloat16
LOG2E = 1.4426950408889634


def shift(value, axis, count, by):
    return lax.ppermute(value, axis, [(i, (i + by) % count) for i in range(count)])


def exchange(value, axis):
    return lax.all_to_all(value, axis, 0, 0, tiled=True)


def both_ways(value):
    pairs = []
    for z in range(NZ):
        pairs += [(z * NC, (z + 1) % NZ * NC), (z * NC + 1, (z - 1) % NZ * NC + 1)]
    return lax.ppermute(value, ("z", "c"), pairs)


def spread_z(piece):
    found = [piece]
    message = jnp.stack([piece, shift(piece, "c", NC, 1)])
    for _ in range(1, NZ // 2):
        message = both_ways(message)
        found += [message, shift(message[1], "c", NC, 1)]
    found.append(both_ways(message[0]))
    return found


def spread_y(piece):
    half = NZ // 2
    right = shift(piece, "y", NY, 1)
    left = shift(piece, "y", NY, -1)
    return [piece, right, left, shift(right[:half], "y", NY, 1), shift(left[half:], "y", NY, -1)]


def dot(a, b):
    return lax.dot_general(a, b, (((1,), (0,)), ((), ())), preferred_element_type=F32)


def dot_nt(a, b):
    return lax.dot_general(a, b, (((1,), (1,)), ((), ())), preferred_element_type=F32)


def dot_tn(a, b):
    return lax.dot_general(a, b, (((0,), (0,)), ((), ())), preferred_element_type=F32)


def inverse_rms(square_sum, width):
    return lax.rsqrt(square_sum * (1.0 / width) + EPS)


def squares(values):
    return jnp.sum(values * values, axis=-1, keepdims=True)


def call(body, outs, args, scratch=(), specs=None, flops=1 << 20, grid=()):
    whole = pl.BlockSpec(memory_space=pltpu.VMEM)
    single = not isinstance(outs, list)
    return pl.pallas_call(
        body,
        out_shape=outs,
        grid=grid,
        in_specs=[whole if specs is None or specs[i] is None else specs[i] for i in range(len(args))],
        out_specs=whole if single else [whole] * len(outs),
        scratch_shapes=list(scratch),
        cost_estimate=pl.CostEstimate(flops=flops, bytes_accessed=1 << 20, transcendentals=0),
    )(*args)


def made(shape, dtype):
    return jax.ShapeDtypeStruct(shape, dtype)


def prep_low_kernel(qd, ld, out):
    x = lax.axis_index("x")
    n = qd.shape[0]
    for j in range(NC):
        out[0, j, :, :] = jnp.zeros((n, 256), BF)
        for i in range(NX):

            @pl.when(x == i)
            def _():
                e = i * NC + j
                out[0, j, :, 0:64] = qd[:, e * Q8 : e * Q8 + 64]
                out[0, j, :, 64:128] = ld[:, e * KV8 : (e + 1) * KV8]
                out[0, j, :, 128:160] = qd[:, e * Q8 + 64 : (e + 1) * Q8]

        ready = out[0, j, :, :]
        for k in range(1, NZ):
            out[k, j, :, :] = ready


def prep_kernel(after, cq, fg, bg, cv, og, co, ao, out):
    for j in range(NC):
        lanes = slice(j * HEAD, (j + 1) * HEAD)
        for k in range(NZ):
            for i, w in enumerate((co, ao, cq, fg, bg, cv, og)):
                out[k, j, :, i * HEAD : (i + 1) * HEAD] = w[:, lanes]


def ups_kernel(q_up, kv_up, q_gain, kv_gain, wq, wkv, gq, gkv):
    c, x = lax.axis_index("c"), lax.axis_index("x")
    for i in range(8):
        e = lax.rem(x - i // NC + NX, NX) * NC + (c if i % NC == 0 else 1 - c)
        row = pl.multiple_of(e * Q8, 32)
        for part, size, at in ((0, 64, i * 64), (64, 32, 512 + i * 32)):
            rows = q_up[pl.ds(row + part, size), :]
            wq[at : at + size, :] = jnp.where(c == 0, rows[:, 0:QK], rows[:, QK : 2 * QK])
            gq[:, at : at + size] = q_gain[pl.ds(e, 1), part : part + size]
        row = pl.multiple_of(e * KV8, 64)
        lanes = pl.ds(pl.multiple_of(c * 256, 256), 256)
        wkv[i * 64 : (i + 1) * 64, :] = kv_up[pl.ds(row, 64), lanes]
        gkv[:, i * 64 : (i + 1) * 64] = kv_gain[pl.ds(e, 1), :]


def gather_rows(scr, sems, refs, lanes):
    y = lax.axis_index("y")
    half = NZ // 2
    copies = []
    for i, (ref, back, rows) in enumerate(
        zip(refs, (0, 1, 3, 2, 2), (None, None, None, slice(0, half), slice(half, NZ)))
    ):
        spot = scr.at[:, lax.rem(y - back + NY, NY)]
        if rows is not None:
            spot = scr.at[rows, lax.rem(y - back + NY, NY)]
        copies.append(pltpu.make_async_copy(ref.at[:, :, lanes], spot, sems.at[i]))
    for copy in copies:
        copy.start()
    return copies


def gathered(scr, copies):
    for copy in copies:
        copy.wait()
    return scr[...].reshape(-1, scr.shape[-1])


def low_kernel(mine, other, gain, rot, b0, b1, b2, b3, b4, normed, low, rotary, w_scr, sems):
    c = lax.axis_index("c")
    copies = gather_rows(w_scr, sems, (b0, b1, b2, b3, b4), slice(0, 256))
    half = mine.shape[0]
    for ref, at in ((mine, c), (other, 1 - c)):
        values = ref[...].astype(F32)
        values = values * inverse_rms(squares(values), values.shape[1]) * gain[...]
        normed[pl.ds(pl.multiple_of(at * half, half), half), :] = values.astype(BF)
    rotary[...] = dot_nt(normed[...], rot[...]).astype(BF)
    ready = dot(normed[...], gathered(w_scr, copies)).astype(BF)
    n = 2 * half
    low[0:n, :] = ready[:, 0:HEAD]
    for k in range(4):
        low[n : n + n // 4, 32 * k : 32 * k + 32] = ready[k * n // 4 : (k + 1) * n // 4, 128:160]


def chain_kernel(
    after,
    rates,
    normed,
    a0,
    a1,
    a2,
    a3,
    a4,
    inside,
    probe_f,
    probe_b,
    gate,
    packet,
    w_scr,
    sems,
):
    copies = gather_rows(w_scr, sems, (a0, a1, a2, a3, a4), slice(256, 896))
    acc = dot(normed[...], gathered(w_scr, copies))
    ready = acc.astype(BF)
    n = ready.shape[0]
    query = ready[:, 0:128].astype(F32)
    payload = ready[:, 384:512]
    gate[...] = ready[:, 512:640]
    row = lax.broadcasted_iota(jnp.int32, (n, n), 0)
    col = lax.broadcasted_iota(jnp.int32, (n, n), 1)
    within = None
    logs = []
    for d in range(2):
        keep = (row >= col) if d == 0 else (row <= col)
        logit = ready[:, 128 * (d + 1) : 128 * (d + 2)].astype(F32)
        key = rates[d : d + 1, :] * jax.nn.sigmoid(-logit)
        log = jnp.log1p(-key)
        high = log.astype(BF)
        rest = (log - high.astype(F32)).astype(BF)
        tri = keep.astype(BF)
        cum = dot(tri, high) + dot(tri, rest)
        total = cum[n - 1 : n, :] if d == 0 else cum[0:1, :]
        probe = (query * jnp.exp(cum)).astype(BF)
        look = (key * jnp.exp(-cum)).astype(BF)
        (probe_f if d == 0 else probe_b)[...] = probe
        score = jnp.where(keep, dot_nt(probe, look), 0.0)
        within = score if within is None else within + score
        digest = dot_tn(payload, (key * jnp.exp(total - cum)).astype(BF)).astype(BF)
        for k in range(NY):
            packet[k, d * HEAD : (d + 1) * HEAD, :] = digest
        high = total.astype(BF).astype(F32)
        logs += [high, total - high]
    inside[...] = dot(within.astype(BF), payload)
    at = lax.broadcasted_iota(jnp.int32, (16, HEAD), 0)
    tail = jnp.zeros((16, HEAD), F32)
    for i, log in enumerate(logs):
        tail = jnp.where(at == i, log, tail)
    tail = tail.astype(BF)
    for k in range(NY):
        packet[k, 2 * HEAD : 2 * HEAD + 16, :] = tail


def walk(states, logs, order, chosen):
    state = jnp.zeros((HEAD, HEAD), F32)
    log = jnp.zeros((1, HEAD), F32)
    for j in order:
        fresh = state * jnp.exp(logs(j)) + states(j)
        passed = chosen(j)
        state = jnp.where(passed, fresh, state)
        log = jnp.where(passed, log + logs(j), log)
    return state, log


def slab_kernel(slab, state_f, state_b, log_out, send):
    z, y = lax.axis_index("z"), lax.axis_index("y")
    at = lax.broadcasted_iota(jnp.int32, (16, HEAD), 0)
    kept = []
    for d in range(2):
        order = range(NY) if d == 0 else range(NY - 1, -1, -1)

        def states(j):
            return slab[j, d * HEAD : (d + 1) * HEAD, :].astype(F32)

        def logs(j):
            block = slab[j, 2 * HEAD : 2 * HEAD + 16, :].astype(F32)
            return block[2 * d : 2 * d + 1, :] + block[2 * d + 1 : 2 * d + 2, :]

        part, log = walk(states, logs, order, (lambda j: j < y) if d == 0 else (lambda j: j > y))
        full, full_log = walk(states, logs, order, lambda j: j >= 0)
        (state_f if d == 0 else state_b)[...] = part
        log_out[d : d + 1, :] = log
        high = full_log.astype(BF).astype(F32)
        tail = jnp.where(at == 0, high, jnp.where(at == 1, full_log - high, 0.0)).astype(BF)
        kept.append((full.astype(BF), tail))
    for k in range(NZ):
        ahead = k > z
        send[k, 0:HEAD, :] = jnp.where(ahead, kept[0][0], kept[1][0])
        send[k, HEAD : HEAD + 16, :] = jnp.where(ahead, kept[0][1], kept[1][1])


def close_kernel(
    outer, state_f, state_b, log_in, probe_f, probe_b, inside, gate, gain, mixed
):
    z = lax.axis_index("z")
    combined = inside[...]
    for d in range(2):
        order = range(NZ) if d == 0 else range(NZ - 1, -1, -1)

        def states(j):
            return outer[j, 0:HEAD, :].astype(F32)

        def logs(j):
            block = outer[j, HEAD : HEAD + 16, :].astype(F32)
            return block[0:1, :] + block[1:2, :]

        far, _ = walk(states, logs, order, (lambda j: j < z) if d == 0 else (lambda j: j > z))
        near = (state_f if d == 0 else state_b)[...]
        state = near + far * jnp.exp(log_in[d : d + 1, :])
        probe = (probe_f if d == 0 else probe_b)[...]
        combined = combined + dot_nt(probe, state.astype(BF))
    opened = gate[...].astype(F32)
    opened = opened * jax.nn.sigmoid(opened)
    scale = inverse_rms(squares(combined), HEAD)
    mixed[...] = (combined * scale * gain[...] * opened).astype(BF)


def heads_kernel(*refs):
    pieces = refs[:8]
    wq, wkv, gq, gkv, rotary, cos, sin, qh_gain, kh_gain = refs[8:17]
    q_out, kv_out, q_scr, kv_scr = refs[17:]
    n = rotary.shape[0]
    half = n // 2
    for i, ref in enumerate(pieces):
        q_scr[:, i * 64 : (i + 1) * 64] = ref[0:n, 0:64]
        kv_scr[:, i * 64 : (i + 1) * 64] = ref[0:n, 64:128]
        for k in range(4):
            rows = slice(k * n // 4, (k + 1) * n // 4)
            q_scr[rows, 512 + 32 * i : 544 + 32 * i] = ref[n : n + n // 4, 32 * k : 32 * k + 32]

    def latent(scr, width, up, gain):
        values = scr[...].astype(F32)
        values = values * inverse_rms(squares(values), width) * gain[...]
        return dot(values.astype(BF), up[...]).astype(BF)

    query = latent(q_scr, QLAT, wq, gq).astype(F32)
    pairs = latent(kv_scr, KVLAT, wkv, gkv)

    def turned(tail):
        swapped = jnp.concatenate([tail[:, ROPE // 2 :], tail[:, : ROPE // 2]], axis=1)
        return (tail * cos[...] + swapped * sin[...]).astype(BF)

    scale = inverse_rms(squares(query), QK)
    query = query * scale * qh_gain[...]
    nope = query[:, 0:HEAD].astype(BF)
    tail = turned(query[:, HEAD:QK])
    for k in range(NY):
        q_out[k, 0:n, :] = nope
        q_out[k, n : n + half, 0:ROPE] = tail[0:half]
        q_out[k, n : n + half, ROPE:HEAD] = tail[half:n]
    key = pairs[:, 0:HEAD].astype(F32)
    rope = rotary[...].astype(F32)
    scale = inverse_rms(squares(key) + squares(rope), QK)
    kv_out[0:n, :] = (key * scale * kh_gain[:, 0:HEAD]).astype(BF)
    kv_out[n : 2 * n, :] = pairs[:, HEAD : 2 * HEAD]
    tail = turned(rope * scale * kh_gain[:, HEAD:QK])
    kv_out[2 * n : 2 * n + half, 0:ROPE] = tail[0:half]
    kv_out[2 * n : 2 * n + half, ROPE:HEAD] = tail[half:n]


def attend_kernel(count, last, queries, *refs):
    kv_refs, rest = refs[:count], refs[count:]
    acc_ref = rest[0] if last else None
    outs = rest[1:-3] if last else rest[0:1]
    q_scr, key_scr, val_scr = rest[-3:]
    y = lax.axis_index("y")
    n = queries.shape[1] * 2 // 3
    half = n // 2
    for i, kv in enumerate(kv_refs):
        at = i * n
        kv = kv.at[0] if len(kv.shape) == 3 else kv
        key_scr[at : at + n, 0:HEAD] = kv[0:n, :]
        tail = kv[2 * n : 2 * n + half, :]
        key_scr[at : at + half, HEAD:QK] = tail[:, 0:ROPE]
        key_scr[at + half : at + n, HEAD:QK] = tail[:, ROPE:HEAD]
        val_scr[at : at + n, 0:HEAD] = kv[n : 2 * n, :]
    val_scr[:, HEAD : 2 * HEAD] = jnp.ones((count * n, HEAD), BF)
    diagonal = lax.broadcasted_iota(jnp.int32, (HEAD, HEAD), 0) == lax.broadcasted_iota(
        jnp.int32, (HEAD, HEAD), 1
    )
    for k in range(NY):
        i = lax.rem(y + k, NY)
        q_scr[0:n, 0:HEAD] = queries[i, 0:n, :]
        tail = queries[i, n : n + half, :]
        q_scr[0:half, HEAD:QK] = tail[:, 0:ROPE]
        q_scr[half:n, HEAD:QK] = tail[:, ROPE:HEAD]
        scores = dot_nt(q_scr[...], key_scr[...])
        weights = jnp.exp2(scores * (QK**-0.5 * LOG2E)).astype(BF)
        sums = dot(weights, val_scr[...])
        if not last:
            outs[0][k] = sums
            continue
        sums = sums + acc_ref[k]
        outs[k][0:n, :] = sums[:, 0:HEAD].astype(BF)
        row = lax.broadcasted_iota(jnp.int32, (16, HEAD), 0)
        tail = jnp.zeros((16, HEAD), F32)
        for b in range(0, n, HEAD):
            size = min(HEAD, n - b)
            den = sums[b : b + size, HEAD : 2 * HEAD]
            line = jnp.sum(jnp.where(diagonal[0:size], den, 0.0), axis=0, keepdims=True)
            high = line.astype(BF).astype(F32)
            tail = jnp.where(row == 2 * (b // HEAD), high, tail)
            tail = jnp.where(row == 2 * (b // HEAD) + 1, line - high, tail)
        outs[k][n : n + 16, :] = tail.astype(BF)


def attend(queries, pieces, acc):
    n = pieces[0].shape[-2] * 2 // 5
    last = acc is not None
    args = [queries] + list(pieces) + ([acc] if last else [])
    count = len(pieces)

    def body(*refs):
        attend_kernel(count, last, *refs)

    def only_first(value):
        if value.ndim == 2:
            return None
        return pl.BlockSpec((1,) + value.shape[1:], lambda i: (0, 0, 0))

    return call(
        body,
        [made((n + 16, HEAD), BF)] * NY if last else made((NY, n, 2 * HEAD), F32),
        args,
        scratch=[
            pltpu.VMEM((n, QK), BF),
            pltpu.VMEM((count * n, QK), BF),
            pltpu.VMEM((count * n, 2 * HEAD), BF),
        ],
        specs=[None] + [only_first(p) for p in pieces] + ([None] if last else []),
        flops=2 * NY * n * count * n * 512,
        grid=(1,),
    )


def final_kernel(
    p0, p1, p2, p3, chain, gain, o0, o1, o2, o3, o4, mine, theirs, scr, w_scr, sems
):
    c, x = lax.axis_index("c"), lax.axis_index("x")
    n = chain.shape[0]
    half = n // 2
    quarter = half // NX
    parts = (p0, p1, p2, p3)
    copies = gather_rows(w_scr, sems, (o0, o1, o2, o3, o4), slice(0, 256))
    sums = lines = None
    for part in parts:
        values = part[0:n, :].astype(F32)
        line = part[n : n + 16, :].astype(F32)
        sums = values if sums is None else sums + values
        lines = line if lines is None else lines + line
    row = lax.broadcasted_iota(jnp.int32, (HEAD, HEAD), 0)
    diagonal = row == lax.broadcasted_iota(jnp.int32, (HEAD, HEAD), 1)
    scr[:, 0:HEAD] = chain[...].astype(F32)
    for b in range(0, n, HEAD):
        size = min(HEAD, n - b)
        i = 2 * (b // HEAD)
        line = lines[i : i + 1, :] + lines[i + 1 : i + 2, :]
        den = jnp.sum(jnp.where(diagonal, line, 0.0), axis=1, keepdims=True)[0:size]
        rows = sums[b : b + size] / den
        scale = inverse_rms(squares(rows), HEAD)
        scr[b : b + size, HEAD : 2 * HEAD] = rows * scale * gain[...]
    weight = gathered(w_scr, copies)
    for out, core in ((mine, c), (theirs, 1 - c)):
        picked = []
        for k in range(NX):
            at = core * half + lax.rem(x + k, NX) * quarter
            picked.append(scr[pl.ds(pl.multiple_of(at, 8), quarter), :])
        mixed = jnp.concatenate(picked, axis=0).astype(BF)
        out[...] = dot_nt(mixed, weight).astype(out.dtype)


def on_device(
    tokens,
    input_gain,
    chain_query,
    forward_gate,
    backward_gate,
    chain_value,
    output_gate,
    forget_rate,
    chain_gain,
    query_down,
    latent_down,
    rotary_down,
    query_latent_gain,
    latent_gain,
    query_up,
    latent_up,
    query_head_gain,
    key_head_gain,
    mixer_gain,
    chain_out,
    attend_out,
):
    z, y, c, _ = (lax.axis_index(a) for a in ("z", "y", "c", "x"))
    rows, width = tokens.shape
    n = rows * NC
    seq_len = n * NY * NZ
    piece = chain_query.shape[0]

    def cols(weight, size):
        return lax.dynamic_slice_in_dim(weight, c * size, size, 1)

    send_b = call(prep_low_kernel, made((NZ, NC, piece, 256), BF), (query_down, latent_down))
    anywhere = pl.BlockSpec(memory_space=pl.ANY)
    send_a = call(
        prep_kernel,
        made((NZ, NC, piece, 896), BF),
        (
            send_b,
            chain_query,
            forward_gate,
            backward_gate,
            chain_value,
            output_gate,
            chain_out.T,
            attend_out.T,
        ),
        specs=[anywhere] + [None] * 7,
    )

    def along_z(value):
        flat = value.reshape(NZ * NC, piece, value.shape[-1])
        return exchange(flat, ("z", "c")).reshape(NZ, NC * piece, value.shape[-1])

    other = shift(tokens, "c", NC, 1)
    column_b = along_z(send_b)
    column_a = along_z(send_a)
    weights_b = spread_y(column_b)
    weights_a = spread_y(column_a)

    positions = ((z * NY + y) * n + jnp.arange(n, dtype=jnp.int32)).astype(F32)
    inverse = THETA ** (-jnp.arange(0, ROPE, 2).astype(F32) / ROPE)
    angles = positions[:, None] * inverse
    cosine, sine = jnp.cos(angles), jnp.sin(angles)
    early = [
        jnp.concatenate([cosine, cosine], axis=1),
        jnp.concatenate([-sine, sine], axis=1),
        cols(forget_rate, HEAD) / seq_len,
        lax.dynamic_slice_in_dim(chain_gain[None], c * HEAD, HEAD, 1),
        lax.dynamic_slice_in_dim(mixer_gain[None], c * HEAD, HEAD, 1),
    ]
    early += call(
        ups_kernel,
        [
            made((QLAT, QK), BF),
            made((KVLAT, 2 * HEAD), BF),
            made((1, QLAT), F32),
            made((1, KVLAT), F32),
        ],
        (query_up, latent_up, query_latent_gain.reshape(8, Q8), latent_gain.reshape(8, KV8)),
    )
    weights_b[4], early = lax.optimization_barrier((weights_b[4], early))
    cos2, sin2, rates, gain_c, gain_m, wq, wkv, gq, gkv = early
    normed, low, rotary = call(
        low_kernel,
        [made((n, width), BF), made((n * 5 // 4, HEAD), BF), made((n, ROPE), BF)],
        [tokens, other, input_gain[None], rotary_down.T] + weights_b,
        scratch=[pltpu.VMEM((NZ, NY, NC * piece, 256), BF), pltpu.SemaphoreType.DMA((5,))],
        specs=[None] * 4 + [anywhere] * 5,
        flops=2 * n * width * 320,
    )
    pieces = []
    for k in range(NX):
        got = low if k == 0 else shift(low, "x", NX, k)
        pieces += [got, shift(got, "c", NC, 1)]
    queries, kv_piece = call(
        heads_kernel,
        [made((NY, n * 3 // 2, HEAD), BF), made((n * 5 // 2, HEAD), BF)],
        pieces
        + [wq, wkv, gq, gkv, rotary, cos2, sin2, query_head_gain[None], key_head_gain[None]],
        scratch=[pltpu.VMEM((n, QLAT), BF), pltpu.VMEM((n, KVLAT), BF)],
        flops=2 * n * (QLAT * QK + KVLAT * 256),
    )
    kv = spread_z(kv_piece)
    all_queries = exchange(queries, "y")
    acc = attend(all_queries, kv[:5], None)
    part = attend(all_queries, kv[5:], acc)
    parts = [part[0]] + [shift(part[k], "y", NY, k) for k in range(1, NY)]

    inside, probe_f, probe_b, gate, packet = call(
        chain_kernel,
        [
            made((n, HEAD), F32),
            made((n, HEAD), BF),
            made((n, HEAD), BF),
            made((n, HEAD), BF),
            made((NY, 2 * HEAD + 16, HEAD), BF),
        ],
        [kv_piece, rates, normed] + weights_a,
        scratch=[pltpu.VMEM((NZ, NY, NC * piece, 640), BF), pltpu.SemaphoreType.DMA((5,))],
        specs=[anywhere, None, None] + [anywhere] * 5,
        flops=2 * n * width * 640,
    )
    slab = exchange(packet, "y")
    state_f, state_b, log_in, send = call(
        slab_kernel,
        [
            made((HEAD, HEAD), F32),
            made((HEAD, HEAD), F32),
            made((2, HEAD), F32),
            made((NZ, HEAD + 16, HEAD), BF),
        ],
        (slab,),
    )
    outer = exchange(send, "z")

    chain_mixed = call(
        close_kernel,
        made((n, HEAD), BF),
        (
            outer,
            state_f,
            state_b,
            log_in,
            probe_f,
            probe_b,
            inside,
            gate,
            gain_c,
        ),
    )
    mine, theirs = call(
        final_kernel,
        [made((rows, width), F32), made((rows, width), BF)],
        parts + [chain_mixed, gain_m] + weights_a,
        scratch=[
            pltpu.VMEM((n, 2 * HEAD), F32),
            pltpu.VMEM((NZ, NY, NC * piece, 256), BF),
            pltpu.SemaphoreType.DMA((5,)),
        ],
        specs=[None] * 6 + [anywhere] * 5,
        flops=2 * n * width * 256,
    )
    summed = mine + shift(theirs, "c", NC, 1).astype(F32)
    quarter = rows // NX
    result = summed[:quarter]
    for k in range(1, NX):
        row = summed[k * quarter : (k + 1) * quarter].astype(BF)
        result = result + shift(row, "x", NX, k).astype(F32)
    return result


def solution(mesh):
    torus = Mesh(mesh.devices.reshape(NZ, NY, NC, NX), ("z", "y", "c", "x"))
    placed = (
        P(SP, None),
        P(),
        P(SP, "x"),
        P(SP, "x"),
        P(SP, "x"),
        P(SP, "x"),
        P(SP, "x"),
        P(None, "x"),
        P("x"),
        P(SP, None),
        P(SP, None),
        P(),
        P(),
        P(),
        P(None, "x"),
        P(None, "x"),
        P(),
        P(),
        P("x"),
        P("x", SP),
        P("x", SP),
    )

    return jax.shard_map(
        on_device, mesh=torus, in_specs=placed, out_specs=P(SP + ("x",), None), check_vma=False
    )
```

```python
import jax
import jax.numpy as jnp
from jax import lax
from jax.experimental import pallas as pl
from jax.experimental.pallas import tpu as pltpu
from jax.sharding import Mesh
from jax.sharding import PartitionSpec as P

HEAD = 128
ROPE = 64
QK = 192
QLAT = 768
KVLAT = 512
Q8 = QLAT // 8
KV8 = KVLAT // 8
NZ, NY, NC, NX = 8, 4, 2, 4
EPS = 1e-06
THETA = 10000.0
SP = ("z", "y", "c")
F32 = jnp.float32
BF = jnp.bfloat16
LOG2E = 1.4426950408889634


def shift(value, axis, count, by):
    return lax.ppermute(value, axis, [(i, (i + by) % count) for i in range(count)])


def exchange(value, axis):
    return lax.all_to_all(value, axis, 0, 0, tiled=True)


def ring_z(piece):
    found = [piece]
    up = down = piece
    for k in range(1, NZ // 2 + 1):
        up = shift(up, "z", NZ, 1)
        found.append(up)
        if k < NZ // 2:
            down = shift(down, "z", NZ, -1)
            found.append(down)
    return found


def spread_y(piece):
    half = NZ // 2
    right = shift(piece, "y", NY, 1)
    left = shift(piece, "y", NY, -1)
    far = shift(right[:half], "y", NY, 1), shift(left[half:], "y", NY, -1)
    return [piece, right, left, *far]


def dot(a, b):
    return lax.dot_general(a, b, (((1,), (0,)), ((), ())), preferred_element_type=F32)


def dot_nt(a, b):
    return lax.dot_general(a, b, (((1,), (1,)), ((), ())), preferred_element_type=F32)


def dot_tn(a, b):
    return lax.dot_general(a, b, (((0,), (0,)), ((), ())), preferred_element_type=F32)


def inverse_rms(square_sum, width):
    return lax.rsqrt(square_sum * (1.0 / width) + EPS)


def squares(values):
    return jnp.sum(values * values, axis=-1, keepdims=True)


def call(body, outs, args, scratch=(), specs=None, flops=1 << 20, grid=()):
    whole = pl.BlockSpec(memory_space=pltpu.VMEM)
    single = not isinstance(outs, list)
    return pl.pallas_call(
        body,
        out_shape=outs,
        grid=grid,
        in_specs=[whole if specs is None or specs[i] is None else specs[i] for i in range(len(args))],
        out_specs=whole if single else [whole] * len(outs),
        scratch_shapes=list(scratch),
        cost_estimate=pl.CostEstimate(flops=flops, bytes_accessed=1 << 20, transcendentals=0),
    )(*args)


def made(shape, dtype):
    return jax.ShapeDtypeStruct(shape, dtype)


def prep_low_kernel(qd, ld, out):
    x = lax.axis_index("x")
    n = qd.shape[0]
    for j in range(NC):
        out[0, j, :, :] = jnp.zeros((n, 256), BF)
        for i in range(NX):

            @pl.when(x == i)
            def _():
                e = i * NC + j
                out[0, j, :, 0:64] = qd[:, e * Q8 : e * Q8 + 64]
                out[0, j, :, 64:128] = ld[:, e * KV8 : (e + 1) * KV8]
                out[0, j, :, 128:160] = qd[:, e * Q8 + 64 : (e + 1) * Q8]

        ready = out[0, j, :, :]
        for k in range(1, NZ):
            out[k, j, :, :] = ready


def prep_kernel(after, cq, fg, bg, cv, og, co, ao, out):
    for j in range(NC):
        lanes = slice(j * HEAD, (j + 1) * HEAD)
        for k in range(NZ):
            for i, w in enumerate((cq, fg, bg, cv, og, co, ao)):
                out[k, j, :, i * HEAD : (i + 1) * HEAD] = w[:, lanes]


def ups_kernel(q_up, kv_up, q_gain, kv_gain, wq, wkv, gq, gkv):
    c, x = lax.axis_index("c"), lax.axis_index("x")
    for i in range(8):
        e = lax.rem(x - i // NC + NX, NX) * NC + (c if i % NC == 0 else 1 - c)
        row = pl.multiple_of(e * Q8, 32)
        for part, size, at in ((0, 64, i * 64), (64, 32, 512 + i * 32)):
            rows = q_up[pl.ds(row + part, size), :]
            wq[at : at + size, :] = jnp.where(c == 0, rows[:, 0:QK], rows[:, QK : 2 * QK])
            gq[:, at : at + size] = q_gain[pl.ds(e, 1), part : part + size]
        row = pl.multiple_of(e * KV8, 64)
        lanes = pl.ds(pl.multiple_of(c * 256, 256), 256)
        wkv[i * 64 : (i + 1) * 64, :] = kv_up[pl.ds(row, 64), lanes]
        gkv[:, i * 64 : (i + 1) * 64] = kv_gain[pl.ds(e, 1), :]


def gather_rows(scr, sems, refs, lanes):
    y = lax.axis_index("y")
    half = NZ // 2
    every = slice(0, NZ)
    copies = []
    if len(refs) == NY:
        plan = [(k, every) for k in range(NY)]
    else:
        plan = [(0, every), (1, every), (3, every), (2, slice(0, half)), (2, slice(half, NZ))]
    for i, (ref, (back, rows)) in enumerate(zip(refs, plan)):
        spot = scr.at[rows, lax.rem(y - back + NY, NY)]
        copies.append(pltpu.make_async_copy(ref.at[:, :, lanes], spot, sems.at[i]))
    for copy in copies:
        copy.start()
    return copies


def gathered(scr, copies):
    for copy in copies:
        copy.wait()
    return scr[...].reshape(-1, scr.shape[-1])


def low_kernel(mine, other, gain, rot, b0, b1, b2, b3, normed, low, rotary, w_scr, sems):
    c = lax.axis_index("c")
    copies = gather_rows(w_scr, sems, (b0, b1, b2, b3), slice(0, 256))
    half = mine.shape[0]
    for ref, at in ((mine, c), (other, 1 - c)):

        def some(i, carry):
            values = ref[pl.ds(pl.multiple_of(i * 32, 32), 32), :].astype(F32)
            values = values * inverse_rms(squares(values), values.shape[1]) * gain[...]
            row = pl.multiple_of(at * half + i * 32, 32)
            normed[pl.ds(row, 32), :] = values.astype(BF)
            return carry

        lax.fori_loop(0, half // 32, some, 0)
    rotary[...] = dot_nt(normed[...], rot[...]).astype(BF)
    ready = dot(normed[...], gathered(w_scr, copies)).astype(BF)
    n = 2 * half
    low[0:n, :] = ready[:, 0:HEAD]
    for k in range(4):
        low[n : n + n // 4, 32 * k : 32 * k + 32] = ready[k * n // 4 : (k + 1) * n // 4, 128:160]


def chain_kernel(
    after,
    rates,
    normed,
    a0,
    a1,
    a2,
    a3,
    a4,
    inside,
    probe_f,
    probe_b,
    packet,
    w_scr,
    sems,
):
    copies = gather_rows(w_scr, sems, (a0, a1, a2, a3, a4), slice(0, 512))
    acc = dot(normed[...], gathered(w_scr, copies))
    ready = acc.astype(BF)
    n = ready.shape[0]
    query = ready[:, 0:128].astype(F32)
    payload = ready[:, 384:512]
    row = lax.broadcasted_iota(jnp.int32, (n, n), 0)
    col = lax.broadcasted_iota(jnp.int32, (n, n), 1)
    within = None
    logs = []
    for d in range(2):
        keep = (row >= col) if d == 0 else (row <= col)
        logit = ready[:, 128 * (d + 1) : 128 * (d + 2)].astype(F32)
        key = rates[d : d + 1, :] * jax.nn.sigmoid(-logit)
        log = jnp.log1p(-key)
        high = log.astype(BF)
        rest = (log - high.astype(F32)).astype(BF)
        tri = keep.astype(BF)
        cum = dot(tri, high) + dot(tri, rest)
        total = cum[n - 1 : n, :] if d == 0 else cum[0:1, :]
        probe = (query * jnp.exp(cum)).astype(BF)
        look = (key * jnp.exp(-cum)).astype(BF)
        (probe_f if d == 0 else probe_b)[...] = probe
        score = jnp.where(keep, dot_nt(probe, look), 0.0)
        within = score if within is None else within + score
        digest = dot_tn(payload, (key * jnp.exp(total - cum)).astype(BF)).astype(BF)
        packet[d * HEAD : (d + 1) * HEAD, :] = digest
        high = total.astype(BF).astype(F32)
        logs += [high, total - high]
    inside[...] = dot(within.astype(BF), payload)
    at = lax.broadcasted_iota(jnp.int32, (16, HEAD), 0)
    tail = jnp.zeros((16, HEAD), F32)
    for i, log in enumerate(logs):
        tail = jnp.where(at == i, log, tail)
    packet[2 * HEAD : 2 * HEAD + 16, :] = tail.astype(BF)


def walk(states, logs, order, chosen):
    state = jnp.zeros((HEAD, HEAD), F32)
    log = jnp.zeros((1, HEAD), F32)
    for j in order:
        fresh = state * jnp.exp(logs(j)) + states(j)
        passed = chosen(j)
        state = jnp.where(passed, fresh, state)
        log = jnp.where(passed, log + logs(j), log)
    return state, log


def slab_kernel(s0, s1, s2, s3, state_f, state_b, log_out, send, slab):
    z, y = lax.axis_index("z"), lax.axis_index("y")
    for k, ref in enumerate((s0, s1, s2, s3)):
        slab[lax.rem(y - k + NY, NY)] = ref[...]
    at = lax.broadcasted_iota(jnp.int32, (16, HEAD), 0)
    kept = []
    for d in range(2):
        order = range(NY) if d == 0 else range(NY - 1, -1, -1)

        def states(j):
            return slab[j, d * HEAD : (d + 1) * HEAD, :].astype(F32)

        def logs(j):
            block = slab[j, 2 * HEAD : 2 * HEAD + 16, :].astype(F32)
            return block[2 * d : 2 * d + 1, :] + block[2 * d + 1 : 2 * d + 2, :]

        part, log = walk(states, logs, order, (lambda j: j < y) if d == 0 else (lambda j: j > y))
        full, full_log = walk(states, logs, order, lambda j: j >= 0)
        (state_f if d == 0 else state_b)[...] = part
        log_out[d : d + 1, :] = log
        high = full_log.astype(BF).astype(F32)
        tail = jnp.where(at == 0, high, jnp.where(at == 1, full_log - high, 0.0)).astype(BF)
        kept.append((full.astype(BF), tail))
    for k in range(NZ):
        ahead = k > z
        send[k, 0:HEAD, :] = jnp.where(ahead, kept[0][0], kept[1][0])
        send[k, HEAD : HEAD + 16, :] = jnp.where(ahead, kept[0][1], kept[1][1])


def close_kernel(
    outer,
    state_f,
    state_b,
    log_in,
    probe_f,
    probe_b,
    inside,
    gain,
    normed,
    l0,
    l1,
    l2,
    l3,
    l4,
    mixed,
    w_scr,
    sems,
):
    copies = gather_rows(w_scr, sems, (l0, l1, l2, l3, l4), slice(0, HEAD))
    z = lax.axis_index("z")
    combined = inside[...]
    for d in range(2):
        order = range(NZ) if d == 0 else range(NZ - 1, -1, -1)

        def states(j):
            return outer[j, 0:HEAD, :].astype(F32)

        def logs(j):
            block = outer[j, HEAD : HEAD + 16, :].astype(F32)
            return block[0:1, :] + block[1:2, :]

        far, _ = walk(states, logs, order, (lambda j: j < z) if d == 0 else (lambda j: j > z))
        near = (state_f if d == 0 else state_b)[...]
        state = near + far * jnp.exp(log_in[d : d + 1, :])
        probe = (probe_f if d == 0 else probe_b)[...]
        combined = combined + dot_nt(probe, state.astype(BF))
    opened = dot(normed[...], gathered(w_scr, copies)).astype(BF).astype(F32)
    opened = opened * jax.nn.sigmoid(opened)
    scale = inverse_rms(squares(combined), HEAD)
    mixed[...] = (combined * scale * gain[...] * opened).astype(BF)


def heads_kernel(*refs):
    swapped, wq, wkv, gq, gkv, rotary, cos, sin, qh_gain, kh_gain = refs[4:14]
    q_out, kv_out, q_scr, kv_scr = refs[14:]
    n = rotary.shape[0]
    half = n // 2
    size = n + n // 4
    for i in range(2 * NX):
        ref = refs[i // 2] if i % 2 == 0 else swapped.at[i // 2 * size : (i // 2 + 1) * size]
        q_scr[:, i * 64 : (i + 1) * 64] = ref[0:n, 0:64]
        kv_scr[:, i * 64 : (i + 1) * 64] = ref[0:n, 64:128]
        for k in range(4):
            rows = slice(k * n // 4, (k + 1) * n // 4)
            q_scr[rows, 512 + 32 * i : 544 + 32 * i] = ref[n : n + n // 4, 32 * k : 32 * k + 32]

    def latent(scr, width, up, gain):
        values = scr[...].astype(F32)
        values = values * inverse_rms(squares(values), width) * gain[...]
        return dot(values.astype(BF), up[...]).astype(BF)

    query = latent(q_scr, QLAT, wq, gq).astype(F32)
    pairs = latent(kv_scr, KVLAT, wkv, gkv)

    def turned(tail):
        swapped = jnp.concatenate([tail[:, ROPE // 2 :], tail[:, : ROPE // 2]], axis=1)
        return (tail * cos[...] + swapped * sin[...]).astype(BF)

    scale = inverse_rms(squares(query), QK)
    query = query * scale * qh_gain[...]
    nope = query[:, 0:HEAD].astype(BF)
    tail = turned(query[:, HEAD:QK])
    for k in range(NY):
        q_out[k, 0:n, :] = nope
        q_out[k, n : n + half, 0:ROPE] = tail[0:half]
        q_out[k, n : n + half, ROPE:HEAD] = tail[half:n]
    key = pairs[:, 0:HEAD].astype(F32)
    rope = rotary[...].astype(F32)
    scale = inverse_rms(squares(key) + squares(rope), QK)
    kv_out[0:n, :] = (key * scale * kh_gain[:, 0:HEAD]).astype(BF)
    kv_out[n : 2 * n, :] = pairs[:, HEAD : 2 * HEAD]
    tail = turned(rope * scale * kh_gain[:, HEAD:QK])
    kv_out[2 * n : 2 * n + half, 0:ROPE] = tail[0:half]
    kv_out[2 * n : 2 * n + half, ROPE:HEAD] = tail[half:n]


def attend_kernel(*refs):
    queries, kv_refs = refs[0], refs[1 : 1 + NZ]
    out, q_scr, key_scr, val_scr = refs[1 + NZ :]
    y = lax.axis_index("y")
    n = queries.shape[1] * 2 // 3
    half = n // 2
    for i, kv in enumerate(kv_refs):
        at = i * n
        key_scr[at : at + n, 0:HEAD] = kv[0:n, :]
        tail = kv[2 * n : 2 * n + half, :]
        key_scr[at : at + half, HEAD:QK] = tail[:, 0:ROPE]
        key_scr[at + half : at + n, HEAD:QK] = tail[:, ROPE:HEAD]
        val_scr[at : at + n, 0:HEAD] = kv[n : 2 * n, :]
    val_scr[:, HEAD : 2 * HEAD] = jnp.ones((NZ * n, HEAD), BF)
    diagonal = lax.broadcasted_iota(jnp.int32, (HEAD, HEAD), 0) == lax.broadcasted_iota(
        jnp.int32, (HEAD, HEAD), 1
    )
    for k in range(NY):
        at = lax.rem(y + k, NY)
        q_scr[k, 0:n, 0:HEAD] = queries[at, 0:n, :]
        tail = queries[at, n : n + half, :]
        q_scr[k, 0:half, HEAD:QK] = tail[:, 0:ROPE]
        q_scr[k, half:n, HEAD:QK] = tail[:, ROPE:HEAD]
    row = lax.broadcasted_iota(jnp.int32, (16, HEAD), 0)

    def one(k, carry):
        scores = dot_nt(q_scr[k], key_scr[...])
        weights = jnp.exp2(scores * (QK**-0.5 * LOG2E)).astype(BF)
        sums = dot(weights, val_scr[...])
        out[k, 0:n, :] = sums[:, 0:HEAD].astype(BF)
        tail = jnp.zeros((16, HEAD), F32)
        for b in range(0, n, HEAD):
            size = min(HEAD, n - b)
            den = sums[b : b + size, HEAD : 2 * HEAD]
            line = jnp.sum(jnp.where(diagonal[0:size], den, 0.0), axis=0, keepdims=True)
            high = line.astype(BF).astype(F32)
            tail = jnp.where(row == 2 * (b // HEAD), high, tail)
            tail = jnp.where(row == 2 * (b // HEAD) + 1, line - high, tail)
        out[k, n : n + 16, :] = tail.astype(BF)
        return carry

    lax.fori_loop(0, NY, one, 0)


def attend(queries, pieces):
    n = pieces[0].shape[0] * 2 // 5
    return call(
        attend_kernel,
        made((NY, n + 16, HEAD), BF),
        [queries] + list(pieces),
        scratch=[
            pltpu.VMEM((NY, n, QK), BF),
            pltpu.VMEM((NZ * n, QK), BF),
            pltpu.VMEM((NZ * n, 2 * HEAD), BF),
        ],
        flops=2 * NY * n * NZ * n * 512,
    )


def final_kernel(
    p0, p1, p2, p3, chain, gain, o0, o1, o2, o3, o4, mine, theirs, scr, w_scr, sems
):
    c, x = lax.axis_index("c"), lax.axis_index("x")
    n = chain.shape[0]
    half = n // 2
    quarter = half // NX
    parts = (p0, p1, p2, p3)
    copies = gather_rows(w_scr, sems, (o0, o1, o2, o3, o4), slice(HEAD, 3 * HEAD))
    sums = lines = None
    for part in parts:
        values = part[0:n, :].astype(F32)
        line = part[n : n + 16, :].astype(F32)
        sums = values if sums is None else sums + values
        lines = line if lines is None else lines + line
    row = lax.broadcasted_iota(jnp.int32, (HEAD, HEAD), 0)
    diagonal = row == lax.broadcasted_iota(jnp.int32, (HEAD, HEAD), 1)
    scr[:, 0:HEAD] = chain[...].astype(F32)
    for b in range(0, n, HEAD):
        size = min(HEAD, n - b)
        i = 2 * (b // HEAD)
        line = lines[i : i + 1, :] + lines[i + 1 : i + 2, :]
        den = jnp.sum(jnp.where(diagonal, line, 0.0), axis=1, keepdims=True)[0:size]
        rows = sums[b : b + size] / den
        scale = inverse_rms(squares(rows), HEAD)
        scr[b : b + size, HEAD : 2 * HEAD] = rows * scale * gain[...]
    weight = gathered(w_scr, copies)
    for out, core in ((mine, c), (theirs, 1 - c)):
        picked = []
        for k in range(NX):
            at = core * half + lax.rem(x + k, NX) * quarter
            picked.append(scr[pl.ds(pl.multiple_of(at, 8), quarter), :])
        mixed = jnp.concatenate(picked, axis=0).astype(BF)
        out[...] = dot_nt(mixed, weight).astype(out.dtype)


def on_device(
    tokens,
    input_gain,
    chain_query,
    forward_gate,
    backward_gate,
    chain_value,
    output_gate,
    forget_rate,
    chain_gain,
    query_down,
    latent_down,
    rotary_down,
    query_latent_gain,
    latent_gain,
    query_up,
    latent_up,
    query_head_gain,
    key_head_gain,
    mixer_gain,
    chain_out,
    attend_out,
):
    z, y, c, _ = (lax.axis_index(a) for a in ("z", "y", "c", "x"))
    rows, width = tokens.shape
    n = rows * NC
    seq_len = n * NY * NZ
    piece = chain_query.shape[0]

    def cols(weight, size):
        return lax.dynamic_slice_in_dim(weight, c * size, size, 1)

    send_b = call(prep_low_kernel, made((NZ, NC, piece, 256), BF), (query_down, latent_down))
    anywhere = pl.BlockSpec(memory_space=pl.ANY)
    send_a = call(
        prep_kernel,
        made((NZ, NC, piece, 896), BF),
        (
            send_b,
            chain_query,
            forward_gate,
            backward_gate,
            chain_value,
            output_gate,
            chain_out.T,
            attend_out.T,
        ),
        specs=[anywhere] + [None] * 7,
    )

    def along_z(value):
        flat = value.reshape(NZ * NC, piece, value.shape[-1])
        return exchange(flat, ("z", "c")).reshape(NZ, NC * piece, value.shape[-1])

    other = shift(tokens, "c", NC, 1)
    column_b = along_z(send_b)
    column_a = along_z(send_a)
    column_a, column_l = column_a[:, :, :512], column_a[:, :, 512:]
    weights_b = [column_b] + [shift(column_b, "y", NY, k) for k in range(1, NY)]
    weights_a = spread_y(column_a)
    weights_l = spread_y(column_l)

    positions = ((z * NY + y) * n + jnp.arange(n, dtype=jnp.int32)).astype(F32)
    inverse = THETA ** (-jnp.arange(0, ROPE, 2).astype(F32) / ROPE)
    angles = positions[:, None] * inverse
    cosine, sine = jnp.cos(angles), jnp.sin(angles)
    early = [
        jnp.concatenate([cosine, cosine], axis=1),
        jnp.concatenate([-sine, sine], axis=1),
        cols(forget_rate, HEAD) / seq_len,
        lax.dynamic_slice_in_dim(chain_gain[None], c * HEAD, HEAD, 1),
        lax.dynamic_slice_in_dim(mixer_gain[None], c * HEAD, HEAD, 1),
    ]
    early += call(
        ups_kernel,
        [
            made((QLAT, QK), BF),
            made((KVLAT, 2 * HEAD), BF),
            made((1, QLAT), F32),
            made((1, KVLAT), F32),
        ],
        (query_up, latent_up, query_latent_gain.reshape(8, Q8), latent_gain.reshape(8, KV8)),
    )
    weights_b[3], early = lax.optimization_barrier((weights_b[3], early))
    cos2, sin2, rates, gain_c, gain_m, wq, wkv, gq, gkv = early
    normed, low, rotary = call(
        low_kernel,
        [made((n, width), BF), made((n * 5 // 4, HEAD), BF), made((n, ROPE), BF)],
        [tokens, other, input_gain[None], rotary_down.T] + weights_b,
        scratch=[pltpu.VMEM((NZ, NY, NC * piece, 256), BF), pltpu.SemaphoreType.DMA((4,))],
        specs=[None] * 4 + [anywhere] * 4,
        flops=2 * n * width * 320,
    )
    pieces = [low] + [shift(low, "x", NX, k) for k in range(1, NX)]
    swapped = shift(jnp.concatenate(pieces, axis=0), "c", NC, 1)
    queries, kv_piece = call(
        heads_kernel,
        [made((NY, n * 3 // 2, HEAD), BF), made((n * 5 // 2, HEAD), BF)],
        pieces
        + [swapped, wq, wkv, gq, gkv, rotary, cos2, sin2, query_head_gain[None], key_head_gain[None]],
        scratch=[pltpu.VMEM((n, QLAT), BF), pltpu.VMEM((n, KVLAT), BF)],
        flops=2 * n * (QLAT * QK + KVLAT * 256),
    )
    kv = ring_z(kv_piece)
    all_queries = exchange(queries, "y")
    part = attend(all_queries, kv)
    parts = [part[0]] + [shift(part[k], "y", NY, k) for k in range(1, NY)]

    inside, probe_f, probe_b, packet = call(
        chain_kernel,
        [
            made((n, HEAD), F32),
            made((n, HEAD), BF),
            made((n, HEAD), BF),
            made((2 * HEAD + 16, HEAD), BF),
        ],
        [kv_piece, rates, normed] + weights_a,
        scratch=[pltpu.VMEM((NZ, NY, NC * piece, 512), BF), pltpu.SemaphoreType.DMA((5,))],
        specs=[anywhere, None, None] + [anywhere] * 5,
        flops=2 * n * width * 512,
    )
    slab = [packet] + [shift(packet, "y", NY, k) for k in range(1, NY)]
    state_f, state_b, log_in, send = call(
        slab_kernel,
        [
            made((HEAD, HEAD), F32),
            made((HEAD, HEAD), F32),
            made((2, HEAD), F32),
            made((NZ, HEAD + 16, HEAD), BF),
        ],
        slab,
        scratch=[pltpu.VMEM((NY, 2 * HEAD + 16, HEAD), BF)],
    )
    outer = exchange(send, "z")

    chain_mixed = call(
        close_kernel,
        made((n, HEAD), BF),
        (
            outer,
            state_f,
            state_b,
            log_in,
            probe_f,
            probe_b,
            inside,
            gain_c,
            normed,
            *weights_l,
        ),
        scratch=[pltpu.VMEM((NZ, NY, NC * piece, HEAD), BF), pltpu.SemaphoreType.DMA((5,))],
        specs=[None] * 9 + [anywhere] * 5,
    )
    mine, theirs = call(
        final_kernel,
        [made((rows, width), F32), made((rows, width), BF)],
        parts + [chain_mixed, gain_m] + weights_l,
        scratch=[
            pltpu.VMEM((n, 2 * HEAD), F32),
            pltpu.VMEM((NZ, NY, NC * piece, 256), BF),
            pltpu.SemaphoreType.DMA((5,)),
        ],
        specs=[None] * 6 + [anywhere] * 5,
        flops=2 * n * width * 256,
    )
    summed = mine + shift(theirs, "c", NC, 1).astype(F32)
    quarter = rows // NX
    result = summed[:quarter]
    for k in range(1, NX):
        row = summed[k * quarter : (k + 1) * quarter].astype(BF)
        result = result + shift(row, "x", NX, k).astype(F32)
    return result


def solution(mesh):
    torus = Mesh(mesh.devices.reshape(NZ, NY, NC, NX), ("z", "y", "c", "x"))
    placed = (
        P(SP, None),
        P(),
        P(SP, "x"),
        P(SP, "x"),
        P(SP, "x"),
        P(SP, "x"),
        P(SP, "x"),
        P(None, "x"),
        P("x"),
        P(SP, None),
        P(SP, None),
        P(),
        P(),
        P(),
        P(None, "x"),
        P(None, "x"),
        P(),
        P(),
        P("x"),
        P("x", SP),
        P("x", SP),
    )

    return jax.shard_map(
        on_device, mesh=torus, in_specs=placed, out_specs=P(SP + ("x",), None), check_vma=False
    )
```

```python
import jax
import jax.numpy as jnp
from jax import lax
from jax.experimental import pallas as pl
from jax.experimental.pallas import tpu as pltpu
from jax.sharding import Mesh
from jax.sharding import PartitionSpec as P

HEAD = 128
ROPE = 64
QK = 192
QLAT = 768
KVLAT = 512
Q8 = QLAT // 8
KV8 = KVLAT // 8
NZ, NY, NC, NX = 8, 4, 2, 4
EPS = 1e-06
THETA = 10000.0
SP = ("z", "y", "c")
F32 = jnp.float32
BF = jnp.bfloat16
VMEM_GRANT = 20 << 20
LOG2E = 1.4426950408889634


def shift(value, axis, count, by):
    return lax.ppermute(value, axis, [(i, (i + by) % count) for i in range(count)])


def exchange(value, axis):
    return lax.all_to_all(value, axis, 0, 0, tiled=True)


def ring_z(piece):
    found = [piece]
    up = down = piece
    for k in range(1, NZ // 2 + 1):
        up = shift(up, "z", NZ, 1)
        found.append(up)
        if k < NZ // 2:
            down = shift(down, "z", NZ, -1)
            found.append(down)
    return found


def spread_y(piece):
    half = NZ // 2
    right = shift(piece, "y", NY, 1)
    left = shift(piece, "y", NY, -1)
    far = shift(right[:half], "y", NY, 1), shift(left[half:], "y", NY, -1)
    return [piece, right, left, *far]


def dot(a, b):
    return lax.dot_general(a, b, (((1,), (0,)), ((), ())), preferred_element_type=F32)


def dot_nt(a, b):
    return lax.dot_general(a, b, (((1,), (1,)), ((), ())), preferred_element_type=F32)


def dot_tn(a, b):
    return lax.dot_general(a, b, (((0,), (0,)), ((), ())), preferred_element_type=F32)


def inverse_rms(square_sum, width):
    return lax.rsqrt(square_sum * (1.0 / width) + EPS)


def squares(values):
    return jnp.sum(values * values, axis=-1, keepdims=True)


def call(body, outs, args, scratch=(), specs=None, flops=1 << 20, grid=()):
    whole = pl.BlockSpec(memory_space=pltpu.VMEM)
    single = not isinstance(outs, list)
    return pl.pallas_call(
        body,
        out_shape=outs,
        grid=grid,
        in_specs=[whole if specs is None or specs[i] is None else specs[i] for i in range(len(args))],
        out_specs=whole if single else [whole] * len(outs),
        scratch_shapes=list(scratch),
        cost_estimate=pl.CostEstimate(flops=flops, bytes_accessed=1 << 20, transcendentals=0),
        compiler_params=pltpu.CompilerParams(vmem_limit_bytes=VMEM_GRANT),
    )(*args)


def made(shape, dtype):
    return jax.ShapeDtypeStruct(shape, dtype)


def prep_low_kernel(qd, ld, out):
    x = lax.axis_index("x")
    n = qd.shape[0]
    half = n // 2
    for j in range(NC):
        out[0, j, n : n + half, :] = jnp.zeros((half, HEAD), BF)
        for i in range(NX):

            @pl.when(x == i)
            def _():
                e = i * NC + j
                out[0, j, 0:n, 0:64] = qd[:, e * Q8 : e * Q8 + 64]
                out[0, j, 0:n, 64:128] = ld[:, e * KV8 : (e + 1) * KV8]
                for g in range(2):
                    rows = slice(g * half, (g + 1) * half)
                    lanes = slice(32 * g, 32 * g + 32)
                    out[0, j, n : n + half, lanes] = qd[rows, e * Q8 + 64 : (e + 1) * Q8]

        ready = out[0, j, :, :]
        for k in range(1, NZ):
            out[k, j, :, :] = ready


def prep_kernel(after, cq, fg, bg, cv, og, co, ao, out):
    for j in range(NC):
        lanes = slice(j * HEAD, (j + 1) * HEAD)
        for k in range(NZ):
            for i, w in enumerate((cq, fg, bg, cv, og, co, ao)):
                out[k, j, :, i * HEAD : (i + 1) * HEAD] = w[:, lanes]


def ups_kernel(q_up, kv_up, q_gain, kv_gain, wq, wkv, gq, gkv):
    c, x = lax.axis_index("c"), lax.axis_index("x")
    for i in range(8):
        e = lax.rem(x - i // NC + NX, NX) * NC + (c if i % NC == 0 else 1 - c)
        row = pl.multiple_of(e * Q8, 32)
        for part, size, at in ((0, 64, i * 64), (64, 32, 512 + i * 32)):
            rows = q_up[pl.ds(row + part, size), :]
            wq[at : at + size, :] = jnp.where(c == 0, rows[:, 0:QK], rows[:, QK : 2 * QK])
            gq[:, at : at + size] = q_gain[pl.ds(e, 1), part : part + size]
        row = pl.multiple_of(e * KV8, 64)
        lanes = pl.ds(pl.multiple_of(c * 256, 256), 256)
        wkv[i * 64 : (i + 1) * 64, :] = kv_up[pl.ds(row, 64), lanes]
        gkv[:, i * 64 : (i + 1) * 64] = kv_gain[pl.ds(e, 1), :]


def gather_rows(scr, sems, refs, lanes):
    y = lax.axis_index("y")
    half = NZ // 2
    every = slice(0, NZ)
    copies = []
    if len(refs) == NY:
        plan = [(k, every) for k in range(NY)]
    else:
        plan = [(0, every), (1, every), (3, every), (2, slice(0, half)), (2, slice(half, NZ))]
    for i, (ref, (back, rows)) in enumerate(zip(refs, plan)):
        spot = scr.at[rows, lax.rem(y - back + NY, NY)]
        copies.append(pltpu.make_async_copy(ref.at[:, :, lanes], spot, sems.at[i]))
    for copy in copies:
        copy.start()
    return copies


def gathered(scr, copies):
    for copy in copies:
        copy.wait()
    return scr[...].reshape(-1, scr.shape[-1])


def low_kernel(mine, other, gain, rot, b0, b1, b2, b3, normed, low, rotary, p_scr, w_scr, sems):
    c = lax.axis_index("c")
    copies = gather_rows(p_scr, sems, (b0, b1, b2, b3), slice(0, HEAD))
    half = mine.shape[0]
    for ref, at in ((mine, c), (other, 1 - c)):

        def some(i, carry):
            values = ref[pl.ds(pl.multiple_of(i * 32, 32), 32), :].astype(F32)
            values = values * inverse_rms(squares(values), values.shape[1]) * gain[...]
            row = pl.multiple_of(at * half + i * 32, 32)
            normed[pl.ds(row, 32), :] = values.astype(BF)
            return carry

        lax.fori_loop(0, half // 32, some, 0)
    rotary[...] = dot_nt(normed[...], rot[...]).astype(BF)
    for copy in copies:
        copy.wait()
    size = w_scr.shape[0] // (NZ * NY * NC)
    for i in range(NZ):
        for j in range(NY):
            for k in range(NC):
                at = (i * NY * NC + j * NC + k) * size
                top = k * size * 3 // 2
                w_scr[at : at + size, 0:HEAD] = p_scr[i, j, top : top + size, :]
                rest = p_scr[i, j, top + size : top + size * 3 // 2, :]
                for g in range(2):
                    row = at + g * size // 2
                    w_scr[row : row + size // 2, HEAD : HEAD + 32] = rest[:, 32 * g : 32 * g + 32]
    ready = dot(normed[...], w_scr[...]).astype(BF)
    n = 2 * half
    low[0:n, :] = ready[:, 0:HEAD]
    for k in range(4):
        low[n : n + n // 4, 32 * k : 32 * k + 32] = ready[k * n // 4 : (k + 1) * n // 4, HEAD : HEAD + 32]


def chain_kernel(
    after,
    rates,
    normed,
    a0,
    a1,
    a2,
    a3,
    a4,
    inside,
    probe_f,
    probe_b,
    packet,
    w_scr,
    sems,
):
    copies = gather_rows(w_scr, sems, (a0, a1, a2, a3, a4), slice(0, 512))
    acc = dot(normed[...], gathered(w_scr, copies))
    ready = acc.astype(BF)
    n = ready.shape[0]
    query = ready[:, 0:128].astype(F32)
    payload = ready[:, 384:512]
    row = lax.broadcasted_iota(jnp.int32, (n, n), 0)
    col = lax.broadcasted_iota(jnp.int32, (n, n), 1)
    within = None
    logs = []
    for d in range(2):
        keep = (row >= col) if d == 0 else (row <= col)
        logit = ready[:, 128 * (d + 1) : 128 * (d + 2)].astype(F32)
        key = rates[d : d + 1, :] * jax.nn.sigmoid(-logit)
        log = jnp.log1p(-key)
        high = log.astype(BF)
        rest = (log - high.astype(F32)).astype(BF)
        tri = keep.astype(BF)
        cum = dot(tri, high) + dot(tri, rest)
        total = cum[n - 1 : n, :] if d == 0 else cum[0:1, :]
        probe = (query * jnp.exp(cum)).astype(BF)
        look = (key * jnp.exp(-cum)).astype(BF)
        (probe_f if d == 0 else probe_b)[...] = probe
        score = jnp.where(keep, dot_nt(probe, look), 0.0)
        within = score if within is None else within + score
        digest = dot_tn(payload, (key * jnp.exp(total - cum)).astype(BF)).astype(BF)
        for k in range(NY):
            packet[k, d * HEAD : (d + 1) * HEAD, :] = digest
        high = total.astype(BF).astype(F32)
        logs += [high, total - high]
    inside[...] = dot(within.astype(BF), payload)
    at = lax.broadcasted_iota(jnp.int32, (16, HEAD), 0)
    tail = jnp.zeros((16, HEAD), F32)
    for i, log in enumerate(logs):
        tail = jnp.where(at == i, log, tail)
    for k in range(NY):
        packet[k, 2 * HEAD : 2 * HEAD + 16, :] = tail.astype(BF)


def walk(states, logs, order, chosen):
    state = jnp.zeros((HEAD, HEAD), F32)
    log = jnp.zeros((1, HEAD), F32)
    for j in order:
        fresh = state * jnp.exp(logs(j)) + states(j)
        passed = chosen(j)
        state = jnp.where(passed, fresh, state)
        log = jnp.where(passed, log + logs(j), log)
    return state, log


def slab_kernel(slab, state_f, state_b, log_out, send):
    z, y = lax.axis_index("z"), lax.axis_index("y")
    at = lax.broadcasted_iota(jnp.int32, (16, HEAD), 0)
    kept = []
    for d in range(2):
        order = range(NY) if d == 0 else range(NY - 1, -1, -1)

        def states(j):
            return slab[j, d * HEAD : (d + 1) * HEAD, :].astype(F32)

        def logs(j):
            block = slab[j, 2 * HEAD : 2 * HEAD + 16, :].astype(F32)
            return block[2 * d : 2 * d + 1, :] + block[2 * d + 1 : 2 * d + 2, :]

        part, log = walk(states, logs, order, (lambda j: j < y) if d == 0 else (lambda j: j > y))
        full, full_log = walk(states, logs, order, lambda j: j >= 0)
        (state_f if d == 0 else state_b)[...] = part
        log_out[d : d + 1, :] = log
        high = full_log.astype(BF).astype(F32)
        tail = jnp.where(at == 0, high, jnp.where(at == 1, full_log - high, 0.0)).astype(BF)
        kept.append((full.astype(BF), tail))
    for k in range(NZ):
        ahead = k > z
        send[k, 0:HEAD, :] = jnp.where(ahead, kept[0][0], kept[1][0])
        send[k, HEAD : HEAD + 16, :] = jnp.where(ahead, kept[0][1], kept[1][1])


def close_kernel(
    outer,
    state_f,
    state_b,
    log_in,
    probe_f,
    probe_b,
    inside,
    gain,
    normed,
    l0,
    l1,
    l2,
    l3,
    mixed,
    w_scr,
    sems,
):
    copies = gather_rows(w_scr, sems, (l0, l1, l2, l3), slice(0, HEAD))
    z = lax.axis_index("z")
    combined = inside[...]
    for d in range(2):
        order = range(NZ) if d == 0 else range(NZ - 1, -1, -1)

        def states(j):
            return outer[j, 0:HEAD, :].astype(F32)

        def logs(j):
            block = outer[j, HEAD : HEAD + 16, :].astype(F32)
            return block[0:1, :] + block[1:2, :]

        far, _ = walk(states, logs, order, (lambda j: j < z) if d == 0 else (lambda j: j > z))
        near = (state_f if d == 0 else state_b)[...]
        state = near + far * jnp.exp(log_in[d : d + 1, :])
        probe = (probe_f if d == 0 else probe_b)[...]
        combined = combined + dot_nt(probe, state.astype(BF))
    opened = dot(normed[...], gathered(w_scr, copies)).astype(BF).astype(F32)
    opened = opened * jax.nn.sigmoid(opened)
    scale = inverse_rms(squares(combined), HEAD)
    mixed[...] = (combined * scale * gain[...] * opened).astype(BF)


def heads_kernel(*refs):
    swapped, wq, wkv, gq, gkv, rotary, cos, sin, qh_gain, kh_gain = refs[4:14]
    q_out, kv_out, q_scr, kv_scr = refs[14:]
    n = rotary.shape[0]
    half = n // 2
    size = n + n // 4
    for i in range(2 * NX):
        ref = refs[i // 2] if i % 2 == 0 else swapped.at[i // 2 * size : (i // 2 + 1) * size]
        q_scr[:, i * 64 : (i + 1) * 64] = ref[0:n, 0:64]
        kv_scr[:, i * 64 : (i + 1) * 64] = ref[0:n, 64:128]
        for k in range(4):
            rows = slice(k * n // 4, (k + 1) * n // 4)
            q_scr[rows, 512 + 32 * i : 544 + 32 * i] = ref[n : n + n // 4, 32 * k : 32 * k + 32]

    def latent(scr, width, up, gain):
        values = scr[...].astype(F32)
        values = values * inverse_rms(squares(values), width) * gain[...]
        return dot(values.astype(BF), up[...]).astype(BF)

    query = latent(q_scr, QLAT, wq, gq).astype(F32)
    pairs = latent(kv_scr, KVLAT, wkv, gkv)

    def turned(tail):
        swapped = jnp.concatenate([tail[:, ROPE // 2 :], tail[:, : ROPE // 2]], axis=1)
        return (tail * cos[...] + swapped * sin[...]).astype(BF)

    scale = inverse_rms(squares(query), QK)
    query = query * scale * qh_gain[...]
    nope = query[:, 0:HEAD].astype(BF)
    tail = turned(query[:, HEAD:QK])
    for k in range(NY):
        q_out[k, 0:n, :] = nope
        q_out[k, n : n + half, 0:ROPE] = tail[0:half]
        q_out[k, n : n + half, ROPE:HEAD] = tail[half:n]
    key = pairs[:, 0:HEAD].astype(F32)
    rope = rotary[...].astype(F32)
    scale = inverse_rms(squares(key) + squares(rope), QK)
    kv_out[0:n, :] = (key * scale * kh_gain[:, 0:HEAD]).astype(BF)
    kv_out[n : 2 * n, :] = pairs[:, HEAD : 2 * HEAD]
    tail = turned(rope * scale * kh_gain[:, HEAD:QK])
    kv_out[2 * n : 2 * n + half, 0:ROPE] = tail[0:half]
    kv_out[2 * n : 2 * n + half, ROPE:HEAD] = tail[half:n]


def attend_kernel(*refs):
    queries, kv_refs = refs[0], refs[1 : 1 + NZ]
    outs = refs[1 + NZ : 1 + NZ + NY]
    q_scr, key_scr, val_scr = refs[1 + NZ + NY :]
    y = lax.axis_index("y")
    n = queries.shape[1] * 2 // 3
    half = n // 2
    for i, kv in enumerate(kv_refs):
        at = i * n
        key_scr[at : at + n, 0:HEAD] = kv[0:n, :]
        tail = kv[2 * n : 2 * n + half, :]
        key_scr[at : at + half, HEAD:QK] = tail[:, 0:ROPE]
        key_scr[at + half : at + n, HEAD:QK] = tail[:, ROPE:HEAD]
        val_scr[at : at + n, 0:HEAD] = kv[n : 2 * n, :]
    val_scr[:, HEAD : 2 * HEAD] = jnp.ones((NZ * n, HEAD), BF)
    diagonal = lax.broadcasted_iota(jnp.int32, (HEAD, HEAD), 0) == lax.broadcasted_iota(
        jnp.int32, (HEAD, HEAD), 1
    )
    row = lax.broadcasted_iota(jnp.int32, (16, HEAD), 0)
    for k, out in enumerate(outs):
        at = lax.rem(y + k, NY)
        q_scr[0:n, 0:HEAD] = queries[at, 0:n, :]
        tail = queries[at, n : n + half, :]
        q_scr[0:half, HEAD:QK] = tail[:, 0:ROPE]
        q_scr[half:n, HEAD:QK] = tail[:, ROPE:HEAD]
        scores = dot_nt(q_scr[...], key_scr[...])
        weights = jnp.exp2(scores * (QK**-0.5 * LOG2E)).astype(BF)
        sums = dot(weights, val_scr[...])
        out[0:n, :] = sums[:, 0:HEAD].astype(BF)
        tail = jnp.zeros((16, HEAD), F32)
        for b in range(0, n, HEAD):
            size = min(HEAD, n - b)
            den = sums[b : b + size, HEAD : 2 * HEAD]
            line = jnp.sum(jnp.where(diagonal[0:size], den, 0.0), axis=0, keepdims=True)
            high = line.astype(BF).astype(F32)
            tail = jnp.where(row == 2 * (b // HEAD), high, tail)
            tail = jnp.where(row == 2 * (b // HEAD) + 1, line - high, tail)
        out[n : n + 16, :] = tail.astype(BF)


def attend(queries, pieces):
    n = pieces[0].shape[0] * 2 // 5
    return call(
        attend_kernel,
        [made((n + 16, HEAD), BF)] * NY,
        [queries] + list(pieces),
        scratch=[
            pltpu.VMEM((n, QK), BF),
            pltpu.VMEM((NZ * n, QK), BF),
            pltpu.VMEM((NZ * n, 2 * HEAD), BF),
        ],
        flops=2 * NY * n * NZ * n * 512,
    )


def final_kernel(
    p0, p1, p2, p3, chain, gain, o0, o1, o2, o3, mine, theirs, scr, w_scr, sems
):
    c, x = lax.axis_index("c"), lax.axis_index("x")
    n = chain.shape[0]
    half = n // 2
    quarter = half // NX
    parts = (p0, p1, p2, p3)
    copies = gather_rows(w_scr, sems, (o0, o1, o2, o3), slice(HEAD, 3 * HEAD))
    sums = lines = None
    for part in parts:
        values = part[0:n, :].astype(F32)
        line = part[n : n + 16, :].astype(F32)
        sums = values if sums is None else sums + values
        lines = line if lines is None else lines + line
    row = lax.broadcasted_iota(jnp.int32, (HEAD, HEAD), 0)
    diagonal = row == lax.broadcasted_iota(jnp.int32, (HEAD, HEAD), 1)
    scr[:, 0:HEAD] = chain[...].astype(F32)
    for b in range(0, n, HEAD):
        size = min(HEAD, n - b)
        i = 2 * (b // HEAD)
        line = lines[i : i + 1, :] + lines[i + 1 : i + 2, :]
        den = jnp.sum(jnp.where(diagonal, line, 0.0), axis=1, keepdims=True)[0:size]
        rows = sums[b : b + size] / den
        scale = inverse_rms(squares(rows), HEAD)
        scr[b : b + size, HEAD : 2 * HEAD] = rows * scale * gain[...]
    weight = gathered(w_scr, copies)
    for out, core in ((mine, c), (theirs, 1 - c)):
        picked = []
        for k in range(NX):
            at = core * half + lax.rem(x + k, NX) * quarter
            picked.append(scr[pl.ds(pl.multiple_of(at, 8), quarter), :])
        mixed = jnp.concatenate(picked, axis=0).astype(BF)
        out[...] = dot_nt(mixed, weight).astype(out.dtype)


def on_device(
    tokens,
    input_gain,
    chain_query,
    forward_gate,
    backward_gate,
    chain_value,
    output_gate,
    forget_rate,
    chain_gain,
    query_down,
    latent_down,
    rotary_down,
    query_latent_gain,
    latent_gain,
    query_up,
    latent_up,
    query_head_gain,
    key_head_gain,
    mixer_gain,
    chain_out,
    attend_out,
):
    z, y, c, _ = (lax.axis_index(a) for a in ("z", "y", "c", "x"))
    rows, width = tokens.shape
    n = rows * NC
    seq_len = n * NY * NZ
    piece = chain_query.shape[0]

    def cols(weight, size):
        return lax.dynamic_slice_in_dim(weight, c * size, size, 1)

    send_b = call(
        prep_low_kernel, made((NZ, NC, piece * 3 // 2, HEAD), BF), (query_down, latent_down)
    )
    anywhere = pl.BlockSpec(memory_space=pl.ANY)
    send_a = call(
        prep_kernel,
        made((NZ, NC, piece, 896), BF),
        (
            send_b,
            chain_query,
            forward_gate,
            backward_gate,
            chain_value,
            output_gate,
            chain_out.T,
            attend_out.T,
        ),
        specs=[anywhere] + [None] * 7,
    )

    def along_z(value):
        flat = value.reshape((NZ * NC,) + value.shape[2:])
        return exchange(flat, ("z", "c")).reshape(NZ, -1, value.shape[-1])

    other = shift(tokens, "c", NC, 1)
    column_b = along_z(send_b)
    column_a = along_z(send_a)
    column_a, column_l = column_a[:, :, :512], column_a[:, :, 512:]
    weights_b = [column_b] + [shift(column_b, "y", NY, k) for k in range(1, NY)]
    weights_a = spread_y(column_a)
    weights_l = [column_l] + [shift(column_l, "y", NY, k) for k in range(1, NY)]

    positions = ((z * NY + y) * n + jnp.arange(n, dtype=jnp.int32)).astype(F32)
    inverse = THETA ** (-jnp.arange(0, ROPE, 2).astype(F32) / ROPE)
    angles = positions[:, None] * inverse
    cosine, sine = jnp.cos(angles), jnp.sin(angles)
    early = [
        jnp.concatenate([cosine, cosine], axis=1),
        jnp.concatenate([-sine, sine], axis=1),
        cols(forget_rate, HEAD) / seq_len,
        lax.dynamic_slice_in_dim(chain_gain[None], c * HEAD, HEAD, 1),
        lax.dynamic_slice_in_dim(mixer_gain[None], c * HEAD, HEAD, 1),
    ]
    early += call(
        ups_kernel,
        [
            made((QLAT, QK), BF),
            made((KVLAT, 2 * HEAD), BF),
            made((1, QLAT), F32),
            made((1, KVLAT), F32),
        ],
        (query_up, latent_up, query_latent_gain.reshape(8, Q8), latent_gain.reshape(8, KV8)),
    )
    weights_b[3], early = lax.optimization_barrier((weights_b[3], early))
    cos2, sin2, rates, gain_c, gain_m, wq, wkv, gq, gkv = early
    normed, low, rotary = call(
        low_kernel,
        [made((n, width), BF), made((n * 5 // 4, HEAD), BF), made((n, ROPE), BF)],
        [tokens, other, input_gain[None], rotary_down.T] + weights_b,
        scratch=[
            pltpu.VMEM((NZ, NY, NC * piece * 3 // 2, HEAD), BF),
            pltpu.VMEM((width, HEAD + 32), BF),
            pltpu.SemaphoreType.DMA((4,)),
        ],
        specs=[None] * 4 + [anywhere] * 4,
        flops=2 * n * width * 320,
    )
    pieces = [low] + [shift(low, "x", NX, k) for k in range(1, NX)]
    swapped = shift(jnp.concatenate(pieces, axis=0), "c", NC, 1)
    queries, kv_piece = call(
        heads_kernel,
        [made((NY, n * 3 // 2, HEAD), BF), made((n * 5 // 2, HEAD), BF)],
        pieces
        + [swapped, wq, wkv, gq, gkv, rotary, cos2, sin2, query_head_gain[None], key_head_gain[None]],
        scratch=[pltpu.VMEM((n, QLAT), BF), pltpu.VMEM((n, KVLAT), BF)],
        flops=2 * n * (QLAT * QK + KVLAT * 256),
    )
    kv = ring_z(kv_piece)
    all_queries = exchange(queries, "y")
    part = attend(all_queries, kv)
    parts = [part[0]] + [shift(part[k], "y", NY, k) for k in range(1, NY)]

    inside, probe_f, probe_b, packet = call(
        chain_kernel,
        [
            made((n, HEAD), F32),
            made((n, HEAD), BF),
            made((n, HEAD), BF),
            made((NY, 2 * HEAD + 16, HEAD), BF),
        ],
        [all_queries, rates, normed] + weights_a,
        scratch=[pltpu.VMEM((NZ, NY, NC * piece, 512), BF), pltpu.SemaphoreType.DMA((5,))],
        specs=[anywhere, None, None] + [anywhere] * 5,
        flops=2 * n * width * 512,
    )
    slab = exchange(packet, "y")
    state_f, state_b, log_in, send = call(
        slab_kernel,
        [
            made((HEAD, HEAD), F32),
            made((HEAD, HEAD), F32),
            made((2, HEAD), F32),
            made((NZ, HEAD + 16, HEAD), BF),
        ],
        (slab,),
    )
    outer = exchange(send, "z")

    chain_mixed = call(
        close_kernel,
        made((n, HEAD), BF),
        (
            outer,
            state_f,
            state_b,
            log_in,
            probe_f,
            probe_b,
            inside,
            gain_c,
            normed,
            *weights_l,
        ),
        scratch=[pltpu.VMEM((NZ, NY, NC * piece, HEAD), BF), pltpu.SemaphoreType.DMA((4,))],
        specs=[None] * 9 + [anywhere] * 4,
    )
    mine, theirs = call(
        final_kernel,
        [made((rows, width), F32), made((rows, width), BF)],
        parts + [chain_mixed, gain_m] + weights_l,
        scratch=[
            pltpu.VMEM((n, 2 * HEAD), F32),
            pltpu.VMEM((NZ, NY, NC * piece, 256), BF),
            pltpu.SemaphoreType.DMA((4,)),
        ],
        specs=[None] * 6 + [anywhere] * 4,
        flops=2 * n * width * 256,
    )
    summed = mine + shift(theirs, "c", NC, 1).astype(F32)
    quarter = rows // NX
    result = summed[:quarter]
    for k in range(1, NX):
        row = summed[k * quarter : (k + 1) * quarter].astype(BF)
        result = result + shift(row, "x", NX, k).astype(F32)
    return result


def solution(mesh):
    torus = Mesh(mesh.devices.reshape(NZ, NY, NC, NX), ("z", "y", "c", "x"))
    placed = (
        P(SP, None),
        P(),
        P(SP, "x"),
        P(SP, "x"),
        P(SP, "x"),
        P(SP, "x"),
        P(SP, "x"),
        P(None, "x"),
        P("x"),
        P(SP, None),
        P(SP, None),
        P(),
        P(),
        P(),
        P(None, "x"),
        P(None, "x"),
        P(),
        P(),
        P("x"),
        P("x", SP),
        P("x", SP),
    )

    return jax.shard_map(
        on_device, mesh=torus, in_specs=placed, out_specs=P(SP + ("x",), None), check_vma=False
    )
```

```python
import jax
import jax.numpy as jnp
from jax import lax
from jax.experimental import pallas as pl
from jax.experimental.pallas import tpu as pltpu
from jax.sharding import Mesh
from jax.sharding import PartitionSpec as P

HEAD = 128
ROPE = 64
QK = 192
QLAT = 768
KVLAT = 512
Q8 = QLAT // 8
KV8 = KVLAT // 8
NZ, NY, NC, NX = 8, 4, 2, 4
EPS = 1e-06
THETA = 10000.0
SP = ("z", "y", "c")
F32 = jnp.float32
BF = jnp.bfloat16
VMEM_GRANT = 20 << 20
LOG2E = 1.4426950408889634


def shift(value, axis, count, by):
    return lax.ppermute(value, axis, [(i, (i + by) % count) for i in range(count)])


def exchange(value, axis):
    return lax.all_to_all(value, axis, 0, 0, tiled=True)


def ring_z(piece):
    found = [piece]
    up = down = piece
    for k in range(1, NZ // 2 + 1):
        up = shift(up, "z", NZ, 1)
        found.append(up)
        if k < NZ // 2:
            down = shift(down, "z", NZ, -1)
            found.append(down)
    return found


def spread_y(piece):
    half = NZ // 2
    right = shift(piece, "y", NY, 1)
    left = shift(piece, "y", NY, -1)
    far = shift(right[:half], "y", NY, 1), shift(left[half:], "y", NY, -1)
    return [piece, right, left, *far]


def dot(a, b):
    return lax.dot_general(a, b, (((1,), (0,)), ((), ())), preferred_element_type=F32)


def dot_nt(a, b):
    return lax.dot_general(a, b, (((1,), (1,)), ((), ())), preferred_element_type=F32)


def dot_tn(a, b):
    return lax.dot_general(a, b, (((0,), (0,)), ((), ())), preferred_element_type=F32)


def inverse_rms(square_sum, width):
    return lax.rsqrt(square_sum * (1.0 / width) + EPS)


def squares(values):
    return jnp.sum(values * values, axis=-1, keepdims=True)


def call(body, outs, args, scratch=(), specs=None, flops=1 << 20, grid=()):
    whole = pl.BlockSpec(memory_space=pltpu.VMEM)
    single = not isinstance(outs, list)
    return pl.pallas_call(
        body,
        out_shape=outs,
        grid=grid,
        in_specs=[whole if specs is None or specs[i] is None else specs[i] for i in range(len(args))],
        out_specs=whole if single else [whole] * len(outs),
        scratch_shapes=list(scratch),
        cost_estimate=pl.CostEstimate(flops=flops, bytes_accessed=1 << 20, transcendentals=0),
        compiler_params=pltpu.CompilerParams(vmem_limit_bytes=VMEM_GRANT),
    )(*args)


def made(shape, dtype):
    return jax.ShapeDtypeStruct(shape, dtype)


def prep_low_kernel(qd, ld, out):
    x = lax.axis_index("x")
    n = qd.shape[0]
    half = n // 2
    for j in range(NC):
        out[0, j, n : n + half, :] = jnp.zeros((half, HEAD), BF)
        for i in range(NX):

            @pl.when(x == i)
            def _():
                e = i * NC + j
                out[0, j, 0:n, 0:64] = qd[:, e * Q8 : e * Q8 + 64]
                out[0, j, 0:n, 64:128] = ld[:, e * KV8 : (e + 1) * KV8]
                for g in range(2):
                    rows = slice(g * half, (g + 1) * half)
                    lanes = slice(32 * g, 32 * g + 32)
                    out[0, j, n : n + half, lanes] = qd[rows, e * Q8 + 64 : (e + 1) * Q8]

        ready = out[0, j, :, :]
        for k in range(1, NZ):
            out[k, j, :, :] = ready


def prep_kernel(after, cq, fg, bg, cv, og, co, ao, out_a, out_l):
    for j in range(NC):
        lanes = slice(j * HEAD, (j + 1) * HEAD)
        for k in range(NZ):
            for i, w in enumerate((cq, fg, bg, cv)):
                out_a[k, j, :, i * HEAD : (i + 1) * HEAD] = w[:, lanes]
            for i, w in enumerate((og, co, ao)):
                out_l[k, j, :, i * HEAD : (i + 1) * HEAD] = w[:, lanes]


def ups_kernel(q_up, kv_up, q_gain, kv_gain, wq, wkv, gq, gkv):
    c, x = lax.axis_index("c"), lax.axis_index("x")
    for i in range(8):
        e = lax.rem(x - i // NC + NX, NX) * NC + (c if i % NC == 0 else 1 - c)
        row = pl.multiple_of(e * Q8, 32)
        for part, size, at in ((0, 64, i * 64), (64, 32, 512 + i * 32)):
            rows = q_up[pl.ds(row + part, size), :]
            wq[at : at + size, :] = jnp.where(c == 0, rows[:, 0:QK], rows[:, QK : 2 * QK])
            gq[:, at : at + size] = q_gain[pl.ds(e, 1), part : part + size]
        row = pl.multiple_of(e * KV8, 64)
        lanes = pl.ds(pl.multiple_of(c * 256, 256), 256)
        wkv[i * 64 : (i + 1) * 64, :] = kv_up[pl.ds(row, 64), lanes]
        gkv[:, i * 64 : (i + 1) * 64] = kv_gain[pl.ds(e, 1), :]


def gather_rows(scr, sems, refs, lanes):
    y = lax.axis_index("y")
    half = NZ // 2
    every = slice(0, NZ)
    copies = []
    if len(refs) == NY:
        plan = [(k, every) for k in range(NY)]
    else:
        plan = [(0, every), (1, every), (3, every), (2, slice(0, half)), (2, slice(half, NZ))]
    for i, (ref, (back, rows)) in enumerate(zip(refs, plan)):
        spot = scr.at[rows, lax.rem(y - back + NY, NY)]
        copies.append(pltpu.make_async_copy(ref.at[:, :, lanes], spot, sems.at[i]))
    for copy in copies:
        copy.start()
    return copies


def gathered(scr, copies):
    for copy in copies:
        copy.wait()
    return scr[...].reshape(-1, scr.shape[-1])


def low_kernel(mine, other, gain, rot, b0, b1, b2, b3, normed, low, rotary, p_scr, w_scr, sems):
    c = lax.axis_index("c")
    copies = gather_rows(p_scr, sems, (b0, b1, b2, b3), slice(0, HEAD))
    half = mine.shape[0]
    for ref, at in ((mine, c), (other, 1 - c)):

        def some(i, carry):
            values = ref[pl.ds(pl.multiple_of(i * 32, 32), 32), :].astype(F32)
            values = values * inverse_rms(squares(values), values.shape[1]) * gain[...]
            row = pl.multiple_of(at * half + i * 32, 32)
            normed[pl.ds(row, 32), :] = values.astype(BF)
            return carry

        lax.fori_loop(0, half // 32, some, 0)
    rotary[...] = dot_nt(normed[...], rot[...]).astype(BF)
    for copy in copies:
        copy.wait()
    size = w_scr.shape[0] // (NZ * NY * NC)
    for i in range(NZ):
        for j in range(NY):
            for k in range(NC):
                at = (i * NY * NC + j * NC + k) * size
                top = k * size * 3 // 2
                w_scr[at : at + size, 0:HEAD] = p_scr[i, j, top : top + size, :]
                rest = p_scr[i, j, top + size : top + size * 3 // 2, :]
                for g in range(2):
                    row = at + g * size // 2
                    w_scr[row : row + size // 2, HEAD : HEAD + 32] = rest[:, 32 * g : 32 * g + 32]
    ready = dot(normed[...], w_scr[...]).astype(BF)
    n = 2 * half
    low[0:n, :] = ready[:, 0:HEAD]
    for k in range(4):
        low[n : n + n // 4, 32 * k : 32 * k + 32] = ready[k * n // 4 : (k + 1) * n // 4, HEAD : HEAD + 32]


def chain_kernel(
    after,
    rates,
    normed,
    a0,
    a1,
    a2,
    a3,
    a4,
    inside,
    probes,
    packet,
    w_scr,
    sems,
):
    copies = gather_rows(w_scr, sems, (a0, a1, a2, a3, a4), slice(0, 512))
    acc = dot(normed[...], gathered(w_scr, copies))
    ready = acc.astype(BF)
    n = ready.shape[0]
    query = ready[:, 0:128].astype(F32)
    payload = ready[:, 384:512]
    row = lax.broadcasted_iota(jnp.int32, (n, n), 0)
    col = lax.broadcasted_iota(jnp.int32, (n, n), 1)
    within = None
    logs = []
    for d in range(2):
        keep = (row >= col) if d == 0 else (row <= col)
        logit = ready[:, 128 * (d + 1) : 128 * (d + 2)].astype(F32)
        key = rates[d : d + 1, :] * jax.nn.sigmoid(-logit)
        log = jnp.log1p(-key)
        high = log.astype(BF)
        rest = (log - high.astype(F32)).astype(BF)
        tri = keep.astype(BF)
        cum = dot(tri, high) + dot(tri, rest)
        total = cum[n - 1 : n, :] if d == 0 else cum[0:1, :]
        probe = (query * jnp.exp(cum)).astype(BF)
        look = (key * jnp.exp(-cum)).astype(BF)
        probes[d] = probe
        score = jnp.where(keep, dot_nt(probe, look), 0.0)
        within = score if within is None else within + score
        digest = dot_tn(payload, (key * jnp.exp(total - cum)).astype(BF)).astype(BF)
        for k in range(NY):
            packet[k, d * HEAD : (d + 1) * HEAD, :] = digest
        high = total.astype(BF).astype(F32)
        logs += [high, total - high]
    inside[...] = dot(within.astype(BF), payload)
    at = lax.broadcasted_iota(jnp.int32, (16, HEAD), 0)
    tail = jnp.zeros((16, HEAD), F32)
    for i, log in enumerate(logs):
        tail = jnp.where(at == i, log, tail)
    for k in range(NY):
        packet[k, 2 * HEAD : 2 * HEAD + 16, :] = tail.astype(BF)


def walk(states, logs, order, chosen):
    state = jnp.zeros((HEAD, HEAD), F32)
    log = jnp.zeros((1, HEAD), F32)
    for j in order:
        fresh = state * jnp.exp(logs(j)) + states(j)
        passed = chosen(j)
        state = jnp.where(passed, fresh, state)
        log = jnp.where(passed, log + logs(j), log)
    return state, log


def slab_kernel(slab, nears, log_out, send):
    z, y = lax.axis_index("z"), lax.axis_index("y")
    at = lax.broadcasted_iota(jnp.int32, (16, HEAD), 0)
    kept = []
    for d in range(2):
        order = range(NY) if d == 0 else range(NY - 1, -1, -1)

        def states(j):
            return slab[j, d * HEAD : (d + 1) * HEAD, :].astype(F32)

        def logs(j):
            block = slab[j, 2 * HEAD : 2 * HEAD + 16, :].astype(F32)
            return block[2 * d : 2 * d + 1, :] + block[2 * d + 1 : 2 * d + 2, :]

        part, log = walk(states, logs, order, (lambda j: j < y) if d == 0 else (lambda j: j > y))
        full, full_log = walk(states, logs, order, lambda j: j >= 0)
        nears[d] = part
        log_out[d : d + 1, :] = log
        high = full_log.astype(BF).astype(F32)
        tail = jnp.where(at == 0, high, jnp.where(at == 1, full_log - high, 0.0)).astype(BF)
        kept.append((full.astype(BF), tail))
    for k in range(NZ):
        ahead = k > z
        send[k, 0:HEAD, :] = jnp.where(ahead, kept[0][0], kept[1][0])
        send[k, HEAD : HEAD + 16, :] = jnp.where(ahead, kept[0][1], kept[1][1])


def close_kernel(
    outer,
    nears,
    log_in,
    probes,
    inside,
    gain,
    normed,
    l0,
    l1,
    l2,
    l3,
    mixed,
    w_scr,
    sems,
):
    copies = gather_rows(w_scr, sems, (l0, l1, l2, l3), slice(0, HEAD))
    z = lax.axis_index("z")
    combined = inside[...]
    for d in range(2):
        order = range(NZ) if d == 0 else range(NZ - 1, -1, -1)

        def states(j):
            return outer[j, 0:HEAD, :].astype(F32)

        def logs(j):
            block = outer[j, HEAD : HEAD + 16, :].astype(F32)
            return block[0:1, :] + block[1:2, :]

        far, _ = walk(states, logs, order, (lambda j: j < z) if d == 0 else (lambda j: j > z))
        state = nears[d] + far * jnp.exp(log_in[d : d + 1, :])
        combined = combined + dot_nt(probes[d], state.astype(BF))
    opened = dot(normed[...], gathered(w_scr, copies)).astype(BF).astype(F32)
    opened = opened * jax.nn.sigmoid(opened)
    scale = inverse_rms(squares(combined), HEAD)
    mixed[...] = (combined * scale * gain[...] * opened).astype(BF)


def heads_kernel(*refs):
    swapped, wq, wkv, gq, gkv, rotary, cos, sin, qh_gain, kh_gain = refs[4:14]
    q_out, kv_out, q_scr, kv_scr = refs[14:]
    n = rotary.shape[0]
    half = n // 2
    size = n + n // 4
    for i in range(2 * NX):
        ref = refs[i // 2] if i % 2 == 0 else swapped.at[i // 2 * size : (i // 2 + 1) * size]
        q_scr[:, i * 64 : (i + 1) * 64] = ref[0:n, 0:64]
        kv_scr[:, i * 64 : (i + 1) * 64] = ref[0:n, 64:128]
        for k in range(4):
            rows = slice(k * n // 4, (k + 1) * n // 4)
            q_scr[rows, 512 + 32 * i : 544 + 32 * i] = ref[n : n + n // 4, 32 * k : 32 * k + 32]

    def latent(scr, width, up, gain):
        values = scr[...].astype(F32)
        values = values * inverse_rms(squares(values), width) * gain[...]
        return dot(values.astype(BF), up[...]).astype(BF)

    query = latent(q_scr, QLAT, wq, gq).astype(F32)
    pairs = latent(kv_scr, KVLAT, wkv, gkv)

    def turned(tail):
        swapped = jnp.concatenate([tail[:, ROPE // 2 :], tail[:, : ROPE // 2]], axis=1)
        return (tail * cos[...] + swapped * sin[...]).astype(BF)

    scale = inverse_rms(squares(query), QK)
    query = query * scale * qh_gain[...]
    nope = query[:, 0:HEAD].astype(BF)
    tail = turned(query[:, HEAD:QK])
    for k in range(NY):
        q_out[k, 0:n, :] = nope
        q_out[k, n : n + half, 0:ROPE] = tail[0:half]
        q_out[k, n : n + half, ROPE:HEAD] = tail[half:n]
    key = pairs[:, 0:HEAD].astype(F32)
    rope = rotary[...].astype(F32)
    scale = inverse_rms(squares(key) + squares(rope), QK)
    kv_out[0:n, :] = (key * scale * kh_gain[:, 0:HEAD]).astype(BF)
    kv_out[n : 2 * n, :] = pairs[:, HEAD : 2 * HEAD]
    tail = turned(rope * scale * kh_gain[:, HEAD:QK])
    kv_out[2 * n : 2 * n + half, 0:ROPE] = tail[0:half]
    kv_out[2 * n : 2 * n + half, ROPE:HEAD] = tail[half:n]


def attend_kernel(*refs):
    queries, kv_refs = refs[0], refs[1 : 1 + NZ]
    outs = refs[1 + NZ : 1 + NZ + NY]
    q_scr, key_scr, val_scr = refs[1 + NZ + NY :]
    y = lax.axis_index("y")
    n = queries.shape[1] * 2 // 3
    half = n // 2
    for i, kv in enumerate(kv_refs):
        at = i * n
        key_scr[at : at + n, 0:HEAD] = kv[0:n, :]
        tail = kv[2 * n : 2 * n + half, :]
        key_scr[at : at + half, HEAD:QK] = tail[:, 0:ROPE]
        key_scr[at + half : at + n, HEAD:QK] = tail[:, ROPE:HEAD]
        val_scr[at : at + n, 0:HEAD] = kv[n : 2 * n, :]
    val_scr[:, HEAD : 2 * HEAD] = jnp.ones((NZ * n, HEAD), BF)
    diagonal = lax.broadcasted_iota(jnp.int32, (HEAD, HEAD), 0) == lax.broadcasted_iota(
        jnp.int32, (HEAD, HEAD), 1
    )
    row = lax.broadcasted_iota(jnp.int32, (16, HEAD), 0)
    for k, out in enumerate(outs):
        at = lax.rem(y + k, NY)
        q_scr[0:n, 0:HEAD] = queries[at, 0:n, :]
        tail = queries[at, n : n + half, :]
        q_scr[0:half, HEAD:QK] = tail[:, 0:ROPE]
        q_scr[half:n, HEAD:QK] = tail[:, ROPE:HEAD]
        scores = dot_nt(q_scr[...], key_scr[...])
        weights = jnp.exp2(scores * (QK**-0.5 * LOG2E)).astype(BF)
        sums = dot(weights, val_scr[...])
        out[0:n, :] = sums[:, 0:HEAD].astype(BF)
        tail = jnp.zeros((16, HEAD), F32)
        for b in range(0, n, HEAD):
            size = min(HEAD, n - b)
            den = sums[b : b + size, HEAD : 2 * HEAD]
            line = jnp.sum(jnp.where(diagonal[0:size], den, 0.0), axis=0, keepdims=True)
            high = line.astype(BF).astype(F32)
            tail = jnp.where(row == 2 * (b // HEAD), high, tail)
            tail = jnp.where(row == 2 * (b // HEAD) + 1, line - high, tail)
        out[n : n + 16, :] = tail.astype(BF)


def attend(queries, pieces):
    n = pieces[0].shape[0] * 2 // 5
    return call(
        attend_kernel,
        [made((n + 16, HEAD), BF)] * NY,
        [queries] + list(pieces),
        scratch=[
            pltpu.VMEM((n, QK), BF),
            pltpu.VMEM((NZ * n, QK), BF),
            pltpu.VMEM((NZ * n, 2 * HEAD), BF),
        ],
        flops=2 * NY * n * NZ * n * 512,
    )


def final_kernel(
    p0, p1, p2, p3, chain, gain, o0, o1, o2, o3, mine, theirs, scr, w_scr, sems
):
    c, x = lax.axis_index("c"), lax.axis_index("x")
    n = chain.shape[0]
    half = n // 2
    quarter = half // NX
    parts = (p0, p1, p2, p3)
    copies = gather_rows(w_scr, sems, (o0, o1, o2, o3), slice(HEAD, 3 * HEAD))
    sums = lines = None
    for part in parts:
        values = part[0:n, :].astype(F32)
        line = part[n : n + 16, :].astype(F32)
        sums = values if sums is None else sums + values
        lines = line if lines is None else lines + line
    row = lax.broadcasted_iota(jnp.int32, (HEAD, HEAD), 0)
    diagonal = row == lax.broadcasted_iota(jnp.int32, (HEAD, HEAD), 1)
    scr[:, 0:HEAD] = chain[...].astype(F32)
    for b in range(0, n, HEAD):
        size = min(HEAD, n - b)
        i = 2 * (b // HEAD)
        line = lines[i : i + 1, :] + lines[i + 1 : i + 2, :]
        den = jnp.sum(jnp.where(diagonal, line, 0.0), axis=1, keepdims=True)[0:size]
        rows = sums[b : b + size] / den
        scale = inverse_rms(squares(rows), HEAD)
        scr[b : b + size, HEAD : 2 * HEAD] = rows * scale * gain[...]
    weight = gathered(w_scr, copies)
    for out, core in ((mine, c), (theirs, 1 - c)):
        picked = []
        for k in range(NX):
            at = core * half + lax.rem(x + k, NX) * quarter
            picked.append(scr[pl.ds(pl.multiple_of(at, 8), quarter), :])
        mixed = jnp.concatenate(picked, axis=0).astype(BF)
        out[...] = dot_nt(mixed, weight).astype(out.dtype)


def on_device(
    tokens,
    input_gain,
    chain_query,
    forward_gate,
    backward_gate,
    chain_value,
    output_gate,
    forget_rate,
    chain_gain,
    query_down,
    latent_down,
    rotary_down,
    query_latent_gain,
    latent_gain,
    query_up,
    latent_up,
    query_head_gain,
    key_head_gain,
    mixer_gain,
    chain_out,
    attend_out,
):
    z, y, c, _ = (lax.axis_index(a) for a in ("z", "y", "c", "x"))
    rows, width = tokens.shape
    n = rows * NC
    seq_len = n * NY * NZ
    piece = chain_query.shape[0]

    def cols(weight, size):
        return lax.dynamic_slice_in_dim(weight, c * size, size, 1)

    send_b = call(
        prep_low_kernel, made((NZ, NC, piece * 3 // 2, HEAD), BF), (query_down, latent_down)
    )
    anywhere = pl.BlockSpec(memory_space=pl.ANY)
    send_a, send_l = call(
        prep_kernel,
        [made((NZ, NC, piece, 512), BF), made((NZ, NC, piece, 384), BF)],
        (
            send_b,
            chain_query,
            forward_gate,
            backward_gate,
            chain_value,
            output_gate,
            chain_out.T,
            attend_out.T,
        ),
        specs=[anywhere] + [None] * 7,
    )

    def along_z(value):
        flat = value.reshape((NZ * NC,) + value.shape[2:])
        return exchange(flat, ("z", "c")).reshape(NZ, -1, value.shape[-1])

    other = shift(tokens, "c", NC, 1)
    column_b = along_z(send_b)
    column_a = along_z(send_a)
    column_l = along_z(send_l)
    weights_b = [column_b] + [shift(column_b, "y", NY, k) for k in range(1, NY)]
    weights_a = spread_y(column_a)

    positions = ((z * NY + y) * n + jnp.arange(n, dtype=jnp.int32)).astype(F32)
    inverse = THETA ** (-jnp.arange(0, ROPE, 2).astype(F32) / ROPE)
    angles = positions[:, None] * inverse
    cosine, sine = jnp.cos(angles), jnp.sin(angles)
    early = [
        jnp.concatenate([cosine, cosine], axis=1),
        jnp.concatenate([-sine, sine], axis=1),
        cols(forget_rate, HEAD) / seq_len,
        lax.dynamic_slice_in_dim(chain_gain[None], c * HEAD, HEAD, 1),
        lax.dynamic_slice_in_dim(mixer_gain[None], c * HEAD, HEAD, 1),
    ]
    early += call(
        ups_kernel,
        [
            made((QLAT, QK), BF),
            made((KVLAT, 2 * HEAD), BF),
            made((1, QLAT), F32),
            made((1, KVLAT), F32),
        ],
        (query_up, latent_up, query_latent_gain.reshape(8, Q8), latent_gain.reshape(8, KV8)),
    )
    weights_b[3], early = lax.optimization_barrier((weights_b[3], early))
    cos2, sin2, rates, gain_c, gain_m, wq, wkv, gq, gkv = early
    normed, low, rotary = call(
        low_kernel,
        [made((n, width), BF), made((n * 5 // 4, HEAD), BF), made((n, ROPE), BF)],
        [tokens, other, input_gain[None], rotary_down.T] + weights_b,
        scratch=[
            pltpu.VMEM((NZ, NY, NC * piece * 3 // 2, HEAD), BF),
            pltpu.VMEM((width, HEAD + 32), BF),
            pltpu.SemaphoreType.DMA((4,)),
        ],
        specs=[None] * 4 + [anywhere] * 4,
        flops=2 * n * width * 320,
    )
    pieces = [low] + [shift(low, "x", NX, k) for k in range(1, NX)]
    swapped = shift(jnp.concatenate(pieces, axis=0), "c", NC, 1)
    queries, kv_piece = call(
        heads_kernel,
        [made((NY, n * 3 // 2, HEAD), BF), made((n * 5 // 2, HEAD), BF)],
        pieces
        + [swapped, wq, wkv, gq, gkv, rotary, cos2, sin2, query_head_gain[None], key_head_gain[None]],
        scratch=[pltpu.VMEM((n, QLAT), BF), pltpu.VMEM((n, KVLAT), BF)],
        flops=2 * n * (QLAT * QK + KVLAT * 256),
    )
    kv = ring_z(kv_piece)
    queries, column_l = lax.optimization_barrier((queries, column_l))
    all_queries = exchange(queries, "y")
    weights_l = [column_l] + [shift(column_l, "y", NY, k) for k in range(1, NY)]

    inside, probes, packet = call(
        chain_kernel,
        [
            made((n, HEAD), F32),
            made((2, n, HEAD), BF),
            made((NY, 2 * HEAD + 16, HEAD), BF),
        ],
        [kv_piece, rates, normed] + weights_a,
        scratch=[pltpu.VMEM((NZ, NY, NC * piece, 512), BF), pltpu.SemaphoreType.DMA((5,))],
        specs=[anywhere, None, None] + [anywhere] * 5,
        flops=2 * n * width * 512,
    )
    packet, all_queries = lax.optimization_barrier((packet, all_queries))
    slab = exchange(packet, "y")
    nears, log_in, send = call(
        slab_kernel,
        [
            made((2, HEAD, HEAD), F32),
            made((2, HEAD), F32),
            made((NZ, HEAD + 16, HEAD), BF),
        ],
        (slab,),
    )
    outer = exchange(send, "z")

    part = attend(all_queries, kv)
    parts = [part[0]] + [shift(part[k], "y", NY, k) for k in range(1, NY)]
    chain_mixed = call(
        close_kernel,
        made((n, HEAD), BF),
        (
            outer,
            nears,
            log_in,
            probes,
            inside,
            gain_c,
            normed,
            *weights_l,
        ),
        scratch=[pltpu.VMEM((NZ, NY, NC * piece, HEAD), BF), pltpu.SemaphoreType.DMA((4,))],
        specs=[None] * 7 + [anywhere] * 4,
    )
    mine, theirs = call(
        final_kernel,
        [made((rows, width), F32), made((rows, width), BF)],
        parts + [chain_mixed, gain_m] + weights_l,
        scratch=[
            pltpu.VMEM((n, 2 * HEAD), F32),
            pltpu.VMEM((NZ, NY, NC * piece, 256), BF),
            pltpu.SemaphoreType.DMA((4,)),
        ],
        specs=[None] * 6 + [anywhere] * 4,
        flops=2 * n * width * 256,
    )
    summed = mine + shift(theirs, "c", NC, 1).astype(F32)
    quarter = rows // NX
    result = summed[:quarter]
    for k in range(1, NX):
        row = summed[k * quarter : (k + 1) * quarter].astype(BF)
        result = result + shift(row, "x", NX, k).astype(F32)
    return result


def solution(mesh):
    torus = Mesh(mesh.devices.reshape(NZ, NY, NC, NX), ("z", "y", "c", "x"))
    placed = (
        P(SP, None),
        P(),
        P(SP, "x"),
        P(SP, "x"),
        P(SP, "x"),
        P(SP, "x"),
        P(SP, "x"),
        P(None, "x"),
        P("x"),
        P(SP, None),
        P(SP, None),
        P(),
        P(),
        P(),
        P(None, "x"),
        P(None, "x"),
        P(),
        P(),
        P("x"),
        P("x", SP),
        P("x", SP),
    )

    return jax.shard_map(
        on_device, mesh=torus, in_specs=placed, out_specs=P(SP + ("x",), None), check_vma=False
    )
```

```python
import jax
import jax.numpy as jnp
from jax import lax
from jax.experimental import pallas as pl
from jax.experimental.pallas import tpu as pltpu
from jax.sharding import Mesh
from jax.sharding import PartitionSpec as P

HEAD = 128
ROPE = 64
QK = 192
QLAT = 768
KVLAT = 512
Q8 = QLAT // 8
KV8 = KVLAT // 8
NZ, NY, NC, NX = 8, 4, 2, 4
EPS = 1e-06
THETA = 10000.0
SP = ("z", "y", "c")
F32 = jnp.float32
BF = jnp.bfloat16
VMEM_GRANT = 20 << 20
WIDE = ("heads",)
LOG2E = 1.4426950408889634


def shift(value, axis, count, by):
    return lax.ppermute(value, axis, [(i, (i + by) % count) for i in range(count)])


def exchange(value, axis):
    return lax.all_to_all(value, axis, 0, 0, tiled=True)


def ring_z(piece):
    found = [piece]
    up = down = piece
    for k in range(1, NZ // 2 + 1):
        up = shift(up, "z", NZ, 1)
        found.append(up)
        if k < NZ // 2:
            down = shift(down, "z", NZ, -1)
            found.append(down)
    return found


def spread_y(piece):
    half = NZ // 2
    right = shift(piece, "y", NY, 1)
    left = shift(piece, "y", NY, -1)
    far = shift(right[:half], "y", NY, 1), shift(left[half:], "y", NY, -1)
    return [piece, right, left, *far]


def dot(a, b):
    return lax.dot_general(a, b, (((1,), (0,)), ((), ())), preferred_element_type=F32)


def dot_nt(a, b):
    return lax.dot_general(a, b, (((1,), (1,)), ((), ())), preferred_element_type=F32)


def dot_tn(a, b):
    return lax.dot_general(a, b, (((0,), (0,)), ((), ())), preferred_element_type=F32)


def inverse_rms(square_sum, width):
    return lax.rsqrt(square_sum * (1.0 / width) + EPS)


def squares(values):
    return jnp.sum(values * values, axis=-1, keepdims=True)


def call(body, outs, args, name, scratch=(), specs=None, flops=1 << 20, grid=()):
    whole = pl.BlockSpec(memory_space=pltpu.VMEM)
    single = not isinstance(outs, list)
    return pl.pallas_call(
        body,
        out_shape=outs,
        grid=grid,
        in_specs=[whole if specs is None or specs[i] is None else specs[i] for i in range(len(args))],
        out_specs=whole if single else [whole] * len(outs),
        scratch_shapes=list(scratch),
        cost_estimate=pl.CostEstimate(flops=flops, bytes_accessed=1 << 20, transcendentals=0),
        compiler_params=pltpu.CompilerParams(
            vmem_limit_bytes=None if name in WIDE else VMEM_GRANT
        ),
    )(*args)


def made(shape, dtype):
    return jax.ShapeDtypeStruct(shape, dtype)


def prep_low_kernel(qd, ld, out):
    x = lax.axis_index("x")
    n = qd.shape[0]
    half = n // 2
    for j in range(NC):
        out[0, j, n : n + half, :] = jnp.zeros((half, HEAD), BF)
        for i in range(NX):

            @pl.when(x == i)
            def _():
                e = i * NC + j
                out[0, j, 0:n, 0:64] = qd[:, e * Q8 : e * Q8 + 64]
                out[0, j, 0:n, 64:128] = ld[:, e * KV8 : (e + 1) * KV8]
                for g in range(2):
                    rows = slice(g * half, (g + 1) * half)
                    lanes = slice(32 * g, 32 * g + 32)
                    out[0, j, n : n + half, lanes] = qd[rows, e * Q8 + 64 : (e + 1) * Q8]

        ready = out[0, j, :, :]
        for k in range(1, NZ):
            out[k, j, :, :] = ready


def prep_kernel(after, cq, fg, bg, cv, og, co, ao, out_a, out_l):
    for j in range(NC):
        lanes = slice(j * HEAD, (j + 1) * HEAD)
        for k in range(NZ):
            for i, w in enumerate((cq, fg, bg, cv)):
                out_a[k, j, :, i * HEAD : (i + 1) * HEAD] = w[:, lanes]
            for i, w in enumerate((og, co, ao)):
                out_l[k, j, :, i * HEAD : (i + 1) * HEAD] = w[:, lanes]


def ups_kernel(q_up, kv_up, q_gain, kv_gain, wq, wkv, gq, gkv):
    c, x = lax.axis_index("c"), lax.axis_index("x")
    for i in range(8):
        e = lax.rem(x - i // NC + NX, NX) * NC + (c if i % NC == 0 else 1 - c)
        row = pl.multiple_of(e * Q8, 32)
        for part, size, at in ((0, 64, i * 64), (64, 32, 512 + i * 32)):
            rows = q_up[pl.ds(row + part, size), :]
            wq[at : at + size, :] = jnp.where(c == 0, rows[:, 0:QK], rows[:, QK : 2 * QK])
            gq[:, at : at + size] = q_gain[pl.ds(e, 1), part : part + size]
        row = pl.multiple_of(e * KV8, 64)
        lanes = pl.ds(pl.multiple_of(c * 256, 256), 256)
        wkv[i * 64 : (i + 1) * 64, :] = kv_up[pl.ds(row, 64), lanes]
        gkv[:, i * 64 : (i + 1) * 64] = kv_gain[pl.ds(e, 1), :]


def gather_rows(scr, sems, refs, lanes):
    y = lax.axis_index("y")
    half = NZ // 2
    every = slice(0, NZ)
    copies = []
    if len(refs) == NY:
        plan = [(k, every) for k in range(NY)]
    else:
        plan = [(0, every), (1, every), (3, every), (2, slice(0, half)), (2, slice(half, NZ))]
    for i, (ref, (back, rows)) in enumerate(zip(refs, plan)):
        spot = scr.at[rows, lax.rem(y - back + NY, NY)]
        copies.append(pltpu.make_async_copy(ref.at[:, :, lanes], spot, sems.at[i]))
    for copy in copies:
        copy.start()
    return copies


def gathered(scr, copies):
    for copy in copies:
        copy.wait()
    return scr[...].reshape(-1, scr.shape[-1])


def low_kernel(mine, other, gain, rot, b0, b1, b2, b3, normed, low, rotary, p_scr, w_scr, sems):
    c = lax.axis_index("c")
    copies = gather_rows(p_scr, sems, (b0, b1, b2, b3), slice(0, HEAD))
    half = mine.shape[0]
    for ref, at in ((mine, c), (other, 1 - c)):

        def some(i, carry):
            values = ref[pl.ds(pl.multiple_of(i * 32, 32), 32), :].astype(F32)
            values = values * inverse_rms(squares(values), values.shape[1]) * gain[...]
            row = pl.multiple_of(at * half + i * 32, 32)
            normed[pl.ds(row, 32), :] = values.astype(BF)
            return carry

        lax.fori_loop(0, half // 32, some, 0)
    rotary[...] = dot_nt(normed[...], rot[...]).astype(BF)
    for copy in copies:
        copy.wait()
    size = w_scr.shape[0] // (NZ * NY * NC)
    for i in range(NZ):
        for j in range(NY):
            for k in range(NC):
                at = (i * NY * NC + j * NC + k) * size
                top = k * size * 3 // 2
                w_scr[at : at + size, 0:HEAD] = p_scr[i, j, top : top + size, :]
                rest = p_scr[i, j, top + size : top + size * 3 // 2, :]
                for g in range(2):
                    row = at + g * size // 2
                    w_scr[row : row + size // 2, HEAD : HEAD + 32] = rest[:, 32 * g : 32 * g + 32]
    ready = dot(normed[...], w_scr[...]).astype(BF)
    n = 2 * half
    low[0:n, :] = ready[:, 0:HEAD]
    for k in range(4):
        low[n : n + n // 4, 32 * k : 32 * k + 32] = ready[k * n // 4 : (k + 1) * n // 4, HEAD : HEAD + 32]


def chain_kernel(
    after,
    rates,
    normed,
    a0,
    a1,
    a2,
    a3,
    a4,
    inside,
    probes,
    packet,
    w_scr,
    sems,
):
    copies = gather_rows(w_scr, sems, (a0, a1, a2, a3, a4), slice(0, 512))
    acc = dot(normed[...], gathered(w_scr, copies))
    ready = acc.astype(BF)
    n = ready.shape[0]
    query = ready[:, 0:128].astype(F32)
    payload = ready[:, 384:512]
    row = lax.broadcasted_iota(jnp.int32, (n, n), 0)
    col = lax.broadcasted_iota(jnp.int32, (n, n), 1)
    within = None
    logs = []
    for d in range(2):
        keep = (row >= col) if d == 0 else (row <= col)
        logit = ready[:, 128 * (d + 1) : 128 * (d + 2)].astype(F32)
        key = rates[d : d + 1, :] * jax.nn.sigmoid(-logit)
        log = jnp.log1p(-key)
        high = log.astype(BF)
        rest = (log - high.astype(F32)).astype(BF)
        tri = keep.astype(BF)
        cum = dot(tri, high) + dot(tri, rest)
        total = cum[n - 1 : n, :] if d == 0 else cum[0:1, :]
        probe = (query * jnp.exp(cum)).astype(BF)
        look = (key * jnp.exp(-cum)).astype(BF)
        probes[d] = probe
        score = jnp.where(keep, dot_nt(probe, look), 0.0)
        within = score if within is None else within + score
        digest = dot_tn(payload, (key * jnp.exp(total - cum)).astype(BF)).astype(BF)
        for k in range(NY):
            packet[k, d * HEAD : (d + 1) * HEAD, :] = digest
        high = total.astype(BF).astype(F32)
        logs += [high, total - high]
    inside[...] = dot(within.astype(BF), payload)
    at = lax.broadcasted_iota(jnp.int32, (16, HEAD), 0)
    tail = jnp.zeros((16, HEAD), F32)
    for i, log in enumerate(logs):
        tail = jnp.where(at == i, log, tail)
    for k in range(NY):
        packet[k, 2 * HEAD : 2 * HEAD + 16, :] = tail.astype(BF)


def walk(states, logs, order, chosen):
    state = jnp.zeros((HEAD, HEAD), F32)
    log = jnp.zeros((1, HEAD), F32)
    for j in order:
        fresh = state * jnp.exp(logs(j)) + states(j)
        passed = chosen(j)
        state = jnp.where(passed, fresh, state)
        log = jnp.where(passed, log + logs(j), log)
    return state, log


def slab_kernel(slab, nears, log_out, send):
    z, y = lax.axis_index("z"), lax.axis_index("y")
    at = lax.broadcasted_iota(jnp.int32, (16, HEAD), 0)
    kept = []
    for d in range(2):
        order = range(NY) if d == 0 else range(NY - 1, -1, -1)

        def states(j):
            return slab[j, d * HEAD : (d + 1) * HEAD, :].astype(F32)

        def logs(j):
            block = slab[j, 2 * HEAD : 2 * HEAD + 16, :].astype(F32)
            return block[2 * d : 2 * d + 1, :] + block[2 * d + 1 : 2 * d + 2, :]

        part, log = walk(states, logs, order, (lambda j: j < y) if d == 0 else (lambda j: j > y))
        full, full_log = walk(states, logs, order, lambda j: j >= 0)
        nears[d] = part
        log_out[d : d + 1, :] = log
        high = full_log.astype(BF).astype(F32)
        tail = jnp.where(at == 0, high, jnp.where(at == 1, full_log - high, 0.0)).astype(BF)
        kept.append((full.astype(BF), tail))
    for k in range(NZ):
        ahead = k > z
        send[k, 0:HEAD, :] = jnp.where(ahead, kept[0][0], kept[1][0])
        send[k, HEAD : HEAD + 16, :] = jnp.where(ahead, kept[0][1], kept[1][1])


def close_kernel(
    outer,
    nears,
    log_in,
    probes,
    inside,
    gain,
    normed,
    l0,
    l1,
    l2,
    l3,
    mixed,
    w_scr,
    sems,
):
    copies = gather_rows(w_scr, sems, (l0, l1, l2, l3), slice(0, HEAD))
    z = lax.axis_index("z")
    combined = inside[...]
    for d in range(2):
        order = range(NZ) if d == 0 else range(NZ - 1, -1, -1)

        def states(j):
            return outer[j, 0:HEAD, :].astype(F32)

        def logs(j):
            block = outer[j, HEAD : HEAD + 16, :].astype(F32)
            return block[0:1, :] + block[1:2, :]

        far, _ = walk(states, logs, order, (lambda j: j < z) if d == 0 else (lambda j: j > z))
        state = nears[d] + far * jnp.exp(log_in[d : d + 1, :])
        combined = combined + dot_nt(probes[d], state.astype(BF))
    opened = dot(normed[...], gathered(w_scr, copies)).astype(BF).astype(F32)
    opened = opened * jax.nn.sigmoid(opened)
    scale = inverse_rms(squares(combined), HEAD)
    mixed[...] = (combined * scale * gain[...] * opened).astype(BF)


def heads_kernel(*refs):
    swapped, wq, wkv, gq, gkv, rotary, cos, sin, qh_gain, kh_gain = refs[4:14]
    q_out, kv_out, q_scr, kv_scr = refs[14:]
    n = rotary.shape[0]
    half = n // 2
    size = n + n // 4
    for i in range(2 * NX):
        ref = refs[i // 2] if i % 2 == 0 else swapped.at[i // 2 * size : (i // 2 + 1) * size]
        q_scr[:, i * 64 : (i + 1) * 64] = ref[0:n, 0:64]
        kv_scr[:, i * 64 : (i + 1) * 64] = ref[0:n, 64:128]
        for k in range(4):
            rows = slice(k * n // 4, (k + 1) * n // 4)
            q_scr[rows, 512 + 32 * i : 544 + 32 * i] = ref[n : n + n // 4, 32 * k : 32 * k + 32]

    def latent(scr, width, up, gain):
        values = scr[...].astype(F32)
        values = values * inverse_rms(squares(values), width) * gain[...]
        return dot(values.astype(BF), up[...]).astype(BF)

    query = latent(q_scr, QLAT, wq, gq).astype(F32)
    pairs = latent(kv_scr, KVLAT, wkv, gkv)

    def turned(tail):
        swapped = jnp.concatenate([tail[:, ROPE // 2 :], tail[:, : ROPE // 2]], axis=1)
        return (tail * cos[...] + swapped * sin[...]).astype(BF)

    scale = inverse_rms(squares(query), QK)
    query = query * scale * qh_gain[...]
    nope = query[:, 0:HEAD].astype(BF)
    tail = turned(query[:, HEAD:QK])
    for k in range(NY):
        q_out[k, 0:n, :] = nope
        q_out[k, n : n + half, 0:ROPE] = tail[0:half]
        q_out[k, n : n + half, ROPE:HEAD] = tail[half:n]
    key = pairs[:, 0:HEAD].astype(F32)
    rope = rotary[...].astype(F32)
    scale = inverse_rms(squares(key) + squares(rope), QK)
    kv_out[0:n, :] = (key * scale * kh_gain[:, 0:HEAD]).astype(BF)
    kv_out[n : 2 * n, :] = pairs[:, HEAD : 2 * HEAD]
    tail = turned(rope * scale * kh_gain[:, HEAD:QK])
    kv_out[2 * n : 2 * n + half, 0:ROPE] = tail[0:half]
    kv_out[2 * n : 2 * n + half, ROPE:HEAD] = tail[half:n]


def attend_kernel(*refs):
    queries, kv_refs = refs[0], refs[1 : 1 + NZ]
    outs = refs[1 + NZ : 1 + NZ + NY]
    q_scr, key_scr, val_scr = refs[1 + NZ + NY :]
    y = lax.axis_index("y")
    n = queries.shape[1] * 2 // 3
    half = n // 2
    for i, kv in enumerate(kv_refs):
        at = i * n
        key_scr[at : at + n, 0:HEAD] = kv[0:n, :]
        tail = kv[2 * n : 2 * n + half, :]
        key_scr[at : at + half, HEAD:QK] = tail[:, 0:ROPE]
        key_scr[at + half : at + n, HEAD:QK] = tail[:, ROPE:HEAD]
        val_scr[at : at + n, 0:HEAD] = kv[n : 2 * n, :]
    val_scr[:, HEAD : 2 * HEAD] = jnp.ones((NZ * n, HEAD), BF)
    diagonal = lax.broadcasted_iota(jnp.int32, (HEAD, HEAD), 0) == lax.broadcasted_iota(
        jnp.int32, (HEAD, HEAD), 1
    )
    row = lax.broadcasted_iota(jnp.int32, (16, HEAD), 0)
    for k, out in enumerate(outs):
        at = lax.rem(y + k, NY)
        q_scr[0:n, 0:HEAD] = queries[at, 0:n, :]
        tail = queries[at, n : n + half, :]
        q_scr[0:half, HEAD:QK] = tail[:, 0:ROPE]
        q_scr[half:n, HEAD:QK] = tail[:, ROPE:HEAD]
        scores = dot_nt(q_scr[...], key_scr[...])
        weights = jnp.exp2(scores * (QK**-0.5 * LOG2E)).astype(BF)
        sums = dot(weights, val_scr[...])
        out[0:n, :] = sums[:, 0:HEAD].astype(BF)
        tail = jnp.zeros((16, HEAD), F32)
        for b in range(0, n, HEAD):
            size = min(HEAD, n - b)
            den = sums[b : b + size, HEAD : 2 * HEAD]
            line = jnp.sum(jnp.where(diagonal[0:size], den, 0.0), axis=0, keepdims=True)
            high = line.astype(BF).astype(F32)
            tail = jnp.where(row == 2 * (b // HEAD), high, tail)
            tail = jnp.where(row == 2 * (b // HEAD) + 1, line - high, tail)
        out[n : n + 16, :] = tail.astype(BF)


def attend(queries, pieces):
    n = pieces[0].shape[0] * 2 // 5
    return call(
        attend_kernel,
        [made((n + 16, HEAD), BF)] * NY,
        [queries] + list(pieces),
        "attend",
        scratch=[
            pltpu.VMEM((n, QK), BF),
            pltpu.VMEM((NZ * n, QK), BF),
            pltpu.VMEM((NZ * n, 2 * HEAD), BF),
        ],
        flops=2 * NY * n * NZ * n * 512,
    )


def final_kernel(
    p0, p1, p2, p3, chain, gain, o0, o1, o2, o3, mine, theirs, scr, w_scr, sems
):
    c, x = lax.axis_index("c"), lax.axis_index("x")
    n = chain.shape[0]
    half = n // 2
    quarter = half // NX
    parts = (p0, p1, p2, p3)
    copies = gather_rows(w_scr, sems, (o0, o1, o2, o3), slice(HEAD, 3 * HEAD))
    sums = lines = None
    for part in parts:
        values = part[0:n, :].astype(F32)
        line = part[n : n + 16, :].astype(F32)
        sums = values if sums is None else sums + values
        lines = line if lines is None else lines + line
    row = lax.broadcasted_iota(jnp.int32, (HEAD, HEAD), 0)
    diagonal = row == lax.broadcasted_iota(jnp.int32, (HEAD, HEAD), 1)
    scr[:, 0:HEAD] = chain[...].astype(F32)
    for b in range(0, n, HEAD):
        size = min(HEAD, n - b)
        i = 2 * (b // HEAD)
        line = lines[i : i + 1, :] + lines[i + 1 : i + 2, :]
        den = jnp.sum(jnp.where(diagonal, line, 0.0), axis=1, keepdims=True)[0:size]
        rows = sums[b : b + size] / den
        scale = inverse_rms(squares(rows), HEAD)
        scr[b : b + size, HEAD : 2 * HEAD] = rows * scale * gain[...]
    weight = gathered(w_scr, copies)
    for out, core in ((mine, c), (theirs, 1 - c)):
        picked = []
        for k in range(NX):
            at = core * half + lax.rem(x + k, NX) * quarter
            picked.append(scr[pl.ds(pl.multiple_of(at, 8), quarter), :])
        mixed = jnp.concatenate(picked, axis=0).astype(BF)
        out[...] = dot_nt(mixed, weight).astype(out.dtype)


def on_device(
    tokens,
    input_gain,
    chain_query,
    forward_gate,
    backward_gate,
    chain_value,
    output_gate,
    forget_rate,
    chain_gain,
    query_down,
    latent_down,
    rotary_down,
    query_latent_gain,
    latent_gain,
    query_up,
    latent_up,
    query_head_gain,
    key_head_gain,
    mixer_gain,
    chain_out,
    attend_out,
):
    z, y, c, _ = (lax.axis_index(a) for a in ("z", "y", "c", "x"))
    rows, width = tokens.shape
    n = rows * NC
    seq_len = n * NY * NZ
    piece = chain_query.shape[0]

    def cols(weight, size):
        return lax.dynamic_slice_in_dim(weight, c * size, size, 1)

    send_b = call(
        prep_low_kernel,
        made((NZ, NC, piece * 3 // 2, HEAD), BF),
        (query_down, latent_down),
        "prep_b",
    )
    anywhere = pl.BlockSpec(memory_space=pl.ANY)
    send_a, send_l = call(
        prep_kernel,
        [made((NZ, NC, piece, 512), BF), made((NZ, NC, piece, 384), BF)],
        (
            send_b,
            chain_query,
            forward_gate,
            backward_gate,
            chain_value,
            output_gate,
            chain_out.T,
            attend_out.T,
        ),
        "prep_a",
        specs=[anywhere] + [None] * 7,
    )

    def along_z(value):
        flat = value.reshape((NZ * NC,) + value.shape[2:])
        return exchange(flat, ("z", "c")).reshape(NZ, -1, value.shape[-1])

    other = shift(tokens, "c", NC, 1)
    column_b = along_z(send_b)
    column_a = along_z(send_a)
    column_l = along_z(send_l)
    weights_b = [column_b] + [shift(column_b, "y", NY, k) for k in range(1, NY)]
    weights_a = spread_y(column_a)

    positions = ((z * NY + y) * n + jnp.arange(n, dtype=jnp.int32)).astype(F32)
    inverse = THETA ** (-jnp.arange(0, ROPE, 2).astype(F32) / ROPE)
    angles = positions[:, None] * inverse
    cosine, sine = jnp.cos(angles), jnp.sin(angles)
    early = [
        jnp.concatenate([cosine, cosine], axis=1),
        jnp.concatenate([-sine, sine], axis=1),
        cols(forget_rate, HEAD) / seq_len,
        lax.dynamic_slice_in_dim(chain_gain[None], c * HEAD, HEAD, 1),
        lax.dynamic_slice_in_dim(mixer_gain[None], c * HEAD, HEAD, 1),
    ]
    early += call(
        ups_kernel,
        [
            made((QLAT, QK), BF),
            made((KVLAT, 2 * HEAD), BF),
            made((1, QLAT), F32),
            made((1, KVLAT), F32),
        ],
        (query_up, latent_up, query_latent_gain.reshape(8, Q8), latent_gain.reshape(8, KV8)),
        "ups",
    )
    weights_b[3], early = lax.optimization_barrier((weights_b[3], early))
    cos2, sin2, rates, gain_c, gain_m, wq, wkv, gq, gkv = early
    normed, low, rotary = call(
        low_kernel,
        [made((n, width), BF), made((n * 5 // 4, HEAD), BF), made((n, ROPE), BF)],
        [tokens, other, input_gain[None], rotary_down.T] + weights_b,
        "low",
        scratch=[
            pltpu.VMEM((NZ, NY, NC * piece * 3 // 2, HEAD), BF),
            pltpu.VMEM((width, HEAD + 32), BF),
            pltpu.SemaphoreType.DMA((4,)),
        ],
        specs=[None] * 4 + [anywhere] * 4,
        flops=2 * n * width * 320,
    )
    pieces = [low] + [shift(low, "x", NX, k) for k in range(1, NX)]
    swapped = shift(jnp.concatenate(pieces, axis=0), "c", NC, 1)
    queries, kv_piece = call(
        heads_kernel,
        [made((NY, n * 3 // 2, HEAD), BF), made((n * 5 // 2, HEAD), BF)],
        pieces
        + [swapped, wq, wkv, gq, gkv, rotary, cos2, sin2, query_head_gain[None], key_head_gain[None]],
        "heads",
        scratch=[pltpu.VMEM((n, QLAT), BF), pltpu.VMEM((n, KVLAT), BF)],
        flops=2 * n * (QLAT * QK + KVLAT * 256),
    )
    kv = ring_z(kv_piece)
    queries, column_l = lax.optimization_barrier((queries, column_l))
    all_queries = exchange(queries, "y")
    weights_l = [column_l] + [shift(column_l, "y", NY, k) for k in range(1, NY)]

    inside, probes, packet = call(
        chain_kernel,
        [
            made((n, HEAD), F32),
            made((2, n, HEAD), BF),
            made((NY, 2 * HEAD + 16, HEAD), BF),
        ],
        [kv_piece, rates, normed] + weights_a,
        "chain",
        scratch=[pltpu.VMEM((NZ, NY, NC * piece, 512), BF), pltpu.SemaphoreType.DMA((5,))],
        specs=[anywhere, None, None] + [anywhere] * 5,
        flops=2 * n * width * 512,
    )
    packet, all_queries = lax.optimization_barrier((packet, all_queries))
    slab = exchange(packet, "y")
    nears, log_in, send = call(
        slab_kernel,
        [
            made((2, HEAD, HEAD), F32),
            made((2, HEAD), F32),
            made((NZ, HEAD + 16, HEAD), BF),
        ],
        (slab,),
        "slab",
    )
    outer = exchange(send, "z")

    part = attend(all_queries, kv)
    parts = [part[0]] + [shift(part[k], "y", NY, k) for k in range(1, NY)]
    chain_mixed = call(
        close_kernel,
        made((n, HEAD), BF),
        (
            outer,
            nears,
            log_in,
            probes,
            inside,
            gain_c,
            normed,
            *weights_l,
        ),
        "close",
        scratch=[pltpu.VMEM((NZ, NY, NC * piece, HEAD), BF), pltpu.SemaphoreType.DMA((4,))],
        specs=[None] * 7 + [anywhere] * 4,
    )
    mine, theirs = call(
        final_kernel,
        [made((rows, width), F32), made((rows, width), BF)],
        parts + [chain_mixed, gain_m] + weights_l,
        "final",
        scratch=[
            pltpu.VMEM((n, 2 * HEAD), F32),
            pltpu.VMEM((NZ, NY, NC * piece, 256), BF),
            pltpu.SemaphoreType.DMA((4,)),
        ],
        specs=[None] * 6 + [anywhere] * 4,
        flops=2 * n * width * 256,
    )
    summed = mine + shift(theirs, "c", NC, 1).astype(F32)
    quarter = rows // NX
    result = summed[:quarter]
    for k in range(1, NX):
        row = summed[k * quarter : (k + 1) * quarter].astype(BF)
        result = result + shift(row, "x", NX, k).astype(F32)
    return result


def solution(mesh):
    torus = Mesh(mesh.devices.reshape(NZ, NY, NC, NX), ("z", "y", "c", "x"))
    placed = (
        P(SP, None),
        P(),
        P(SP, "x"),
        P(SP, "x"),
        P(SP, "x"),
        P(SP, "x"),
        P(SP, "x"),
        P(None, "x"),
        P("x"),
        P(SP, None),
        P(SP, None),
        P(),
        P(),
        P(),
        P(None, "x"),
        P(None, "x"),
        P(),
        P(),
        P("x"),
        P("x", SP),
        P("x", SP),
    )

    return jax.shard_map(
        on_device, mesh=torus, in_specs=placed, out_specs=P(SP + ("x",), None), check_vma=False
    )
```
